32 devices in a mesh: grp: 2 (over y), ep: 4 (over z), tp: 4 (over x, core).
Axes of the slice: x: 2, y: 2, z: 4, core: 2. Of those that a mesh axis runs over, the one named last changes fastest.
Arguments:
- queries: bfloat16 [1024, 16, 128], P(('grp', 'ep'), 'tp'), parts along dimension 0, may hold values from -6 to 6
- key_vectors: bfloat16 [1024, 16, 128], P(('grp', 'ep'), 'tp'), parts along dimension 0, may hold values from -6 to 6
- values: bfloat16 [1024, 16, 128], P(('grp', 'ep'), 'tp'), parts along dimension 0, may hold values from -6 to 6
- forget_cum: float32 [1024, 16], P('grp', 'tp'), parts along dimension 0, may hold values from -90 to 0, as said below
- query_gain: float32 [128], replicated, may hold values from 0.1 to 5.5
- key_gain: float32 [128], replicated, may hold values from 0.1 to 5.5
- tokens: bfloat16 [4096, 4096], P(('grp', 'ep', 'tp')), parts along dimension 0, may hold values from -6 to 6
- norm_gain: float32 [4096], replicated, may hold values from 0.1 to 1.9
- routes: int32 [4096, 2], P(('grp', 'ep', 'tp')), parts along dimension 0, may hold values from 0 to 127, all different within a row; in each aligned block of 128 rows (0 to 127, 128 to 255, ...) at most 2 rows name the same one
- route_weights: float32 [4096, 2], P(('grp', 'ep', 'tp')), parts along dimension 0, may hold values from 0.3 to 1.2
- expert_gate: bfloat16 [128, 4096, 384], P(('ep', 'tp')), may hold values from -0.09375 to 0.09375
- expert_up: bfloat16 [128, 4096, 384], P(('ep', 'tp')), may hold values from -0.09375 to 0.09375
- expert_down: bfloat16 [128, 384, 4096], P(('ep', 'tp')), may hold values from -0.3125 to 0.3125
- shared_gate: bfloat16 [4096, 192], P(None, 'tp'), may hold values from -0.09375 to 0.09375
- shared_up: bfloat16 [4096, 192], P(None, 'tp'), may hold values from -0.09375 to 0.09375
- shared_down: bfloat16 [192, 4096], P('tp'), may hold values from -0.4375 to 0.4375
Outputs:
- attended: bfloat16 [1024, 16, 128], P(('grp', 'ep'), 'tp'), parts along dimension 0
- routed_output: bfloat16 [4096, 4096], P(('grp', 'ep', 'tp')), parts along dimension 0
The draws below stay inside these ranges and needn't reach their ends.
There are 2 independent parts, one for each index of `grp`. The reference program is written for one: setup_inputs(seed, part) draws one part's arguments, and reference() takes and returns one part's arrays. A program takes and returns all parts, laid end to end along the dimension named above; an argument that names none is the same for every part. Nothing has to cross between parts.
Inputs may be any that keep to these rules, and one draw needn't show every extreme that they name: `routes`: each row names 2 different experts; the rows of one device name every expert exactly 2 times. `forget_cum`: never rises from one position to the next.
All inputs are finite; a program needn't handle non-finite values.
Results may differ from the reference program's by a relative error of at most 0.007.
The reference program's roundings to bfloat16 on the way count: a program that leaves them out, or rounds other values in their place, can miss the bound.
Values may be sent and summed in bfloat16 or wider, within the bound.
A program may use at most 128 MiB of HBM per device.

```python
import math
import jax
import jax.numpy as jnp
import numpy as np
from jax import lax

D = 4096
HEADS = 16
HD = 128
EXPERTS = 128
EF = 384
SF = 192
TOP_K = 2
TOKENS_PER_SHARD = 128
TOK_B = 128
CAP = 2
SEQUENCE_LENGTH = 512
TOKENS_B = 2048
N_EP = 4
N_TP = 4


def query_key_pair(key):
    query_base = jnp.clip(jax.random.normal(jax.random.fold_in(key, 701), (SEQUENCE_LENGTH, HEADS, HD), jnp.float32), -6.0, 6.0)
    key_base = jnp.clip(jax.random.normal(jax.random.fold_in(key, 702), (SEQUENCE_LENGTH, HEADS, HD), jnp.float32), -6.0, 6.0)
    return (query_base, key_base)


def draw_queries(key, part):
    return query_key_pair(key)[0].astype(jnp.bfloat16)


def draw_key_vectors(key, part):
    return query_key_pair(key)[1].astype(jnp.bfloat16)


def gain_sample(key):
    return 1.0 + jnp.clip(0.18 * jax.random.normal(key, (HD,), jnp.float32), -0.9, 0.9)


def draw_query_gain(key, part):
    return gain_sample(jax.random.fold_in(key, 801))


def draw_key_gain(key, part):
    return gain_sample(jax.random.fold_in(key, 802))


def draw_forget_cum(key, part):
    order = jax.random.permutation(jax.random.fold_in(key, 901), HEADS)
    gentle_decay = (order < HEADS // 2).astype(jnp.float32)
    totals = jnp.exp(jax.random.uniform(jax.random.fold_in(key, 902), (HEADS,), jnp.float32, jnp.log(0.3), jnp.log(1.0))) / SEQUENCE_LENGTH
    quick = jnp.exp(jax.random.uniform(jax.random.fold_in(key, 903), (HEADS,), jnp.float32, jnp.log(1.0 / 60.0), jnp.log(1.0 / 25.0)))
    decay_speed = gentle_decay * totals + (1.0 - gentle_decay) * quick
    block_multiplier = jnp.exp(jax.random.uniform(jax.random.fold_in(key, 904), (SEQUENCE_LENGTH // TOKENS_PER_SHARD,), jnp.float32, jnp.log(0.35), jnp.log(2.8)))
    jagged_profile = jax.random.uniform(jax.random.fold_in(key, 905), (SEQUENCE_LENGTH, HEADS), jnp.float32, 0.5, 1.5)
    position_indices = jnp.arange(SEQUENCE_LENGTH)
    spike_position = jax.random.randint(jax.random.fold_in(key, 906), (3,), 0, SEQUENCE_LENGTH)
    spike_magnitude = jax.random.uniform(jax.random.fold_in(key, 907), (3,), jnp.float32, 0.22, 0.69)
    forget_spike = jnp.sum(jnp.where(position_indices[:, None] == spike_position[None, :], spike_magnitude[None, :], 0.0), axis=1)
    forget_logarithm = -(decay_speed[None, :] * jnp.repeat(block_multiplier, TOKENS_PER_SHARD)[:, None] * jagged_profile) - forget_spike[:, None] * gentle_decay[None, :]
    return jnp.cumsum(forget_logarithm, axis=0)


def block_levels(stream_key, shape, shards, least, top_value):
    gain, own = 1.0, jax.random.fold_in(stream_key, 6)
    for dim, parts in shards:
        draws = jnp.exp(jax.random.uniform(jax.random.fold_in(own, dim), (parts,), jnp.float32, least / len(shards), top_value / len(shards)))
        gain = gain * jnp.repeat(draws, shape[dim] // parts).reshape([-1 if axis == dim else 1 for axis in range(len(shape))])
    return gain


def deal_out(own_key, own, number, rows, amount, top, most, lean):
    order = jax.random.permutation(own_key, amount)
    heavy_load, usual = portions_of(amount, rows * top, most, lean, True), portions_of(amount, rows * top, most, lean, False)
    places = jnp.arange(amount)

    def named(sizes, rotation):
        used = int((sizes > 0).sum())
        fixed = max(1, used // 4)
        passed = fixed + (places - fixed + rotation * (used - fixed)) % max(1, amount - fixed)
        return jnp.zeros((amount,), jnp.int32).at[order[jnp.where(places < fixed, places, passed)]].set(jnp.asarray(sizes, jnp.int32))

    sizes = jnp.where(number % 4 == 0, named(heavy_load, number // 4), named(usual, number - number // 4 - 1))
    mixed = jax.random.permutation(jax.random.fold_in(own, 3), amount)
    source_of, taker = mixed[0:amount // 2 * 2:2], mixed[1:amount // 2 * 2:2]
    margin = jnp.minimum(sizes[source_of] - 1, most - sizes[taker]) // 2
    margin = jnp.where((source_of == order[0]) | (taker == order[0]) | (sizes[taker] == 0), 0, jnp.maximum(margin, 0))
    passed = jax.random.randint(jax.random.fold_in(own, 4), (amount // 2,), 0, 1 << 20) % (margin + 1)
    sizes = sizes.at[source_of].add(-passed).at[taker].add(passed)
    items = jnp.searchsorted(jnp.cumsum(sizes), jnp.arange(rows * top), side="right").astype(jnp.int32)
    grid = items.reshape(top, rows).T
    grid = grid[jax.random.permutation(jax.random.fold_in(own, 1), rows)]
    rotation = jax.random.randint(jax.random.fold_in(own, 2), (rows, 1), 0, top)
    return jnp.take_along_axis(grid, (jnp.arange(top)[None, :] + rotation) % top, axis=1)


def portions_of(number_of, total, limit, skew, full):
    loads = [(1 << 20) // math.isqrt(grade ** skew) + 1 for grade in range(1, number_of + 1)]
    largest = limit if full else min(limit, max(-(-total // number_of), total * loads[0] // sum(loads)))
    least = 1 if total - largest >= number_of - 1 else 0
    counts, surplus = [largest] + [least] * (number_of - 1), total - largest - least * (number_of - 1)
    while surplus > 0:
        movable = [i for i in range(1, number_of) if counts[i] < largest] or [i for i in range(1, number_of) if counts[i] < limit]
        mass, budget = sum([loads[i] for i in movable]), surplus
        for i in movable:
            addition = min(limit - counts[i], max(1, budget * loads[i] // mass), surplus)
            counts[i] = counts[i] + addition
            surplus = surplus - addition
    return np.array(counts)


def scatter_about(key, dims, width, most, shards=(), held_as=jnp.bfloat16):
    level = block_levels(key, dims, shards, -0.22, 0.18) if shards else 1.0
    drawn = jax.random.normal(key, dims, jnp.float32) * width * level
    return jnp.minimum(jnp.maximum(drawn, -most), most).astype(held_as)


def setup_inputs(seed: int = 0, part: int = 0) -> dict:
    streams_of = jax.random.split(jax.random.key(seed), 17)
    part_keys = jax.random.split(jax.random.fold_in(streams_of[16], part), 17)
    queries = draw_queries(jax.random.fold_in(jax.random.fold_in(streams_of[16], part), 71), part)
    key_vectors = draw_key_vectors(jax.random.fold_in(jax.random.fold_in(streams_of[16], part), 71), part)
    values = scatter_about(part_keys[2], (SEQUENCE_LENGTH, HEADS, HD), 1.0, 6.0, ((0, 4), (1, 4)))
    forget_cum = draw_forget_cum(jax.random.fold_in(jax.random.fold_in(streams_of[16], part), 71), part)
    query_gain = draw_query_gain(jax.random.fold_in(streams_of[16], 71), part)
    key_gain = draw_key_gain(jax.random.fold_in(streams_of[16], 71), part)
    tokens = scatter_about(part_keys[6], (TOKENS_B, D), 1.0, 6.0, ((0, 16),))
    norm_gain = jnp.clip(1.0 + 0.18 * jax.random.normal(streams_of[7], (D,), jnp.float32), 0.1, 1.9)
    routes_keys = jax.random.split(jax.random.fold_in(part_keys[8], 1), TOKENS_B // TOK_B)
    routes_turns = jax.random.permutation(jax.random.fold_in(part_keys[8], 3), TOKENS_B // TOK_B)
    routes = jax.vmap(lambda own, number: deal_out(jax.random.fold_in(part_keys[8], 2), own, number, TOK_B, EXPERTS, TOP_K, CAP, 0))(routes_keys, routes_turns).reshape((TOKENS_B, TOP_K))
    route_weights = jnp.clip(0.3 + 0.90000004 * jax.random.uniform(part_keys[9], (TOKENS_B, TOP_K), jnp.float32) ** block_levels(part_keys[9], (TOKENS_B, TOP_K), ((0, 16),), -0.2, 0.2), 0.3, 1.2)
    expert_gate = scatter_about(streams_of[10], (EXPERTS, D, EF), D ** -0.5, 0.09375, ((0, 16),))
    expert_up = scatter_about(streams_of[11], (EXPERTS, D, EF), D ** -0.5, 0.09375, ((0, 16),))
    expert_down = scatter_about(streams_of[12], (EXPERTS, EF, D), EF ** -0.5, 0.3125, ((0, 16),))
    shared_gate = scatter_about(streams_of[13], (D, SF), D ** -0.5, 0.09375, ((1, 4),))
    shared_up = scatter_about(streams_of[14], (D, SF), D ** -0.5, 0.09375, ((1, 4),))
    shared_down = scatter_about(streams_of[15], (SF, D), SF ** -0.5, 0.4375, ((0, 4),))
    return {"queries": queries, "key_vectors": key_vectors, "values": values, "forget_cum": forget_cum, "query_gain": query_gain, "key_gain": key_gain, "tokens": tokens, "norm_gain": norm_gain, "routes": routes, "route_weights": route_weights, "expert_gate": expert_gate, "expert_up": expert_up, "expert_down": expert_down, "shared_gate": shared_gate, "shared_up": shared_up, "shared_down": shared_down}


def rms_rows(row_values, gain_vector):
    widened = row_values.astype(jnp.float32)
    inverse = lax.rsqrt(lax.optimization_barrier(jnp.mean(widened * widened, axis=-1, keepdims=True)) + 1e-06)
    return (widened * inverse * gain_vector.astype(jnp.float32)).astype(jnp.bfloat16)

def attention(queries, key_vectors, values, forget_cum, query_gain, key_gain):
    query_norm = lax.optimization_barrier(rms_rows(queries, query_gain)).astype(jnp.float32)
    key_norm = lax.optimization_barrier(rms_rows(key_vectors, key_gain)).astype(jnp.float32)
    value_wide = values.astype(jnp.float32)
    length = queries.shape[0]
    block_rows = 512 if length % 512 == 0 else length
    scale_factor = queries.shape[2] ** (-0.5)
    outputs = []
    for first_row in range(0, length, block_rows):
        stop_row = first_row + block_rows
        scores = jnp.einsum('qhd,khd->hqk', query_norm[first_row:stop_row], key_norm[:stop_row]) * scale_factor
        scores = scores + forget_cum[first_row:stop_row].T[:, :, None] - forget_cum[:stop_row].T[:, None, :]
        allowed = (jnp.arange(stop_row)[None, :] <= jnp.arange(first_row, stop_row)[:, None])[None]
        scores = jnp.where(allowed, scores, -jnp.inf)
        row_max = lax.optimization_barrier(jnp.max(scores, axis=2, keepdims=True))
        weights = jnp.exp(scores - row_max)
        denominator = lax.optimization_barrier(jnp.sum(weights, axis=2))
        probabilities = lax.optimization_barrier(weights.astype(jnp.bfloat16)).astype(jnp.float32)
        mixed_rows = jnp.einsum('hqk,khd->hqd', probabilities, value_wide[:stop_row]) / denominator[:, :, None]
        outputs.append(mixed_rows.transpose(1, 0, 2))
    return jnp.concatenate(outputs, axis=0).astype(jnp.bfloat16)

def mixture(tokens, norm_gain, routes, route_weights, expert_gate, expert_up, expert_down, shared_gate, shared_up, shared_down):
    normed = rms_rows(tokens, norm_gain)
    row_total = tokens.shape[0]
    shared_hidden = (jax.nn.silu(jnp.dot(normed, shared_gate, preferred_element_type=jnp.float32)) * jnp.dot(normed, shared_up, preferred_element_type=jnp.float32)).astype(jnp.bfloat16)
    part_width = shared_down.shape[0] // N_TP
    shared_sum = jnp.zeros((row_total, tokens.shape[1]), jnp.float32)
    for block_index in range(N_TP):
        low = block_index * part_width
        partial_value = jnp.dot(shared_hidden[:, low:low + part_width], shared_down[low:low + part_width], preferred_element_type=jnp.float32)
        shared_sum = shared_sum + lax.optimization_barrier(partial_value.astype(jnp.bfloat16)).astype(jnp.float32)
    shared_out = shared_sum.astype(jnp.bfloat16)
    block_count = N_EP * N_TP
    per_block = routes.reshape(block_count, -1)
    choices_per = per_block.shape[1]
    token_index = (jnp.arange(block_count)[:, None] * (choices_per // TOP_K) + jnp.arange(choices_per)[None, :] // TOP_K).astype(jnp.int32)
    weight_table = route_weights.reshape(block_count, -1)
    one_hot = (per_block[:, :, None] == jnp.arange(EXPERTS)[None, None, :]).astype(jnp.int32)
    slot_rank = lax.optimization_barrier(jnp.sum((jnp.cumsum(one_hot, axis=1) - one_hot) * one_hot, axis=2))

    def one_expert(running_sum, expert_index):
        chosen = per_block == expert_index
        placed = chosen[:, :, None] & (slot_rank[:, :, None] == jnp.arange(CAP)[None, None, :])
        row_ids = lax.optimization_barrier(jnp.sum(jnp.where(placed, token_index[:, :, None], 0), axis=1)).reshape(-1).astype(jnp.int32)
        slot_weight = lax.optimization_barrier(jnp.sum(jnp.where(placed, weight_table[:, :, None], 0.0), axis=1)).reshape(-1)
        picked = normed[row_ids]
        gate_values = jnp.dot(picked, expert_gate[expert_index], preferred_element_type=jnp.float32)
        upward = jnp.dot(picked, expert_up[expert_index], preferred_element_type=jnp.float32)
        hidden = (jax.nn.silu(gate_values) * upward).astype(jnp.bfloat16)
        produced = jnp.dot(hidden, expert_down[expert_index], preferred_element_type=jnp.float32).astype(jnp.bfloat16)
        produced = lax.optimization_barrier(produced).astype(jnp.float32)
        return (running_sum.at[row_ids].add(slot_weight[:, None] * produced), None)
    routed, _ = lax.scan(one_expert, jnp.zeros((row_total, tokens.shape[1]), jnp.float32), jnp.arange(EXPERTS).astype(jnp.int32))
    return (shared_out.astype(jnp.float32) + routed).astype(jnp.bfloat16)

def reference(queries, key_vectors, values, forget_cum, query_gain, key_gain, tokens, norm_gain, routes, route_weights, expert_gate, expert_up, expert_down, shared_gate, shared_up, shared_down):
    attended = attention(queries, key_vectors, values, forget_cum, query_gain, key_gain)
    routed_output = mixture(tokens, norm_gain, routes, route_weights, expert_gate, expert_up, expert_down, shared_gate, shared_up, shared_down)
    return (attended, routed_output)
```

```python
import functools
import jax
import jax.numpy as jnp
from jax import lax
from jax.experimental import pallas as pl
from jax.experimental.pallas import tpu as pltpu
from jax.sharding import PartitionSpec as P

MESH = pl.DeviceIdType.MESH
F32 = jnp.float32
BF16 = jnp.bfloat16
CAP = 2
GROUPS = 2
HALVES = 2
SENDS = 2
RETURNS = 4
SHARED = 4

D = 4096
EXPERTS = 128
TOP_K = 2


def rms_rows(row_values, gain_vector):
    widened = row_values.astype(jnp.float32)
    inverse = lax.rsqrt(jnp.mean(widened * widened, axis=-1, keepdims=True) + 1e-06)
    return (widened * inverse * gain_vector).astype(jnp.bfloat16)


def attend(queries, key_vectors, values, forget_cum, query_gain, key_gain):
    query_norm = rms_rows(queries, query_gain)
    key_norm = rms_rows(key_vectors, key_gain)
    query_rows = query_norm.shape[0]
    head_count = query_norm.shape[1]
    head_size = query_norm.shape[2]
    first_query = lax.axis_index("ep") * query_rows
    query_positions = first_query + lax.iota(jnp.int32, query_rows)
    last_query = first_query + query_rows - 1
    query_cum = lax.dynamic_slice_in_dim(forget_cum, first_query, query_rows, 0).T
    scale_factor = head_size ** (-0.5)
    start_state = (
        jnp.full((head_count, query_rows), -1e30, jnp.float32),
        jnp.zeros((head_count, query_rows), jnp.float32),
        jnp.zeros((head_count, query_rows, head_size), jnp.float32),
    )
    key_part = lax.all_gather(key_norm, "ep", axis=0, tiled=True)
    value_part = lax.all_gather(values, "ep", axis=0, tiled=True)
    piece_rows = key_part.shape[0]

    def compute(inner_state):
        best_score, denominator, accumulated = inner_state
        cum_block = forget_cum.T
        scores = jnp.einsum(
            "qhd,khd->hqk", query_norm, key_part, preferred_element_type=jnp.float32
        )
        scores = scores * scale_factor + query_cum[:, :, None] - cum_block[:, None, :]
        key_positions = lax.iota(jnp.int32, piece_rows)
        allowed = (key_positions[None, :] <= query_positions[:, None])[None]
        scores = jnp.where(allowed, scores, -1e30)
        new_best = jnp.maximum(best_score, jnp.max(scores, axis=2))
        weights = jnp.where(allowed, jnp.exp(scores - new_best[:, :, None]), 0.0)
        denominator = jnp.sum(weights, axis=2)
        product = jnp.einsum(
            "hqk,khd->hqd",
            weights.astype(jnp.bfloat16),
            value_part,
            preferred_element_type=jnp.float32,
        )
        accumulated = product
        return (new_best, denominator, accumulated)

    best_score, denominator, accumulated = lax.cond(
        jnp.int32(0) <= last_query, compute, lambda inner_state: inner_state, start_state
    )
    return (accumulated / denominator[:, :, None]).transpose(1, 0, 2).astype(jnp.bfloat16)


def shared_expert(normed, shared_gate, shared_up, shared_down):
    row_count = normed.shape[0]
    whole_gate, whole_up, whole_down = (
        lax.all_gather(shared_gate, "tp", axis=1, tiled=True),
        lax.all_gather(shared_up, "tp", axis=1, tiled=True),
        lax.all_gather(shared_down, "tp", axis=0, tiled=True),
    )
    block_total = lax.axis_size("tp")
    gate_values = jnp.dot(normed, whole_gate, preferred_element_type=jnp.float32)
    upward = jnp.dot(normed, whole_up, preferred_element_type=jnp.float32)
    hidden_whole = (jax.nn.silu(gate_values) * upward).astype(jnp.bfloat16)
    part_width = whole_down.shape[0] // block_total
    hidden_blocks = hidden_whole.reshape(row_count, block_total, part_width)
    down_blocks = whole_down.reshape(block_total, part_width, whole_down.shape[1])
    partials = jnp.einsum(
        "rnp,npd->nrd", hidden_blocks, down_blocks, preferred_element_type=jnp.float32
    ).astype(jnp.bfloat16)
    return jnp.sum(partials.astype(jnp.float32), axis=0).astype(jnp.bfloat16)


def mixture(
    tokens,
    norm_gain,
    routes,
    route_weights,
    expert_gate,
    expert_up,
    expert_down,
    shared_gate,
    shared_up,
    shared_down,
):
    normed = rms_rows(tokens, norm_gain)
    row_count = tokens.shape[0]
    shared_out = shared_expert(normed, shared_gate, shared_up, shared_down)
    flat_routes = routes.reshape(-1)
    choice_count = flat_routes.shape[0]
    one_hot = (flat_routes[:, None] == lax.iota(jnp.int32, EXPERTS)[None, :]).astype(jnp.int32)
    slot_rank = jnp.sum((jnp.cumsum(one_hot, axis=0) - one_hot) * one_hot, axis=1)
    slot_index = slot_rank * EXPERTS + flat_routes
    slot_ids = lax.iota(jnp.int32, CAP * EXPERTS)
    matches = slot_index[None, :] == slot_ids[:, None]
    source_row = jnp.sum(
        jnp.where(matches, lax.iota(jnp.int32, choice_count)[None, :] // TOP_K, 0), axis=1
    )
    filled = jnp.any(matches, axis=1)
    outgoing = jnp.where(filled[:, None], normed[source_row], jnp.zeros((), jnp.bfloat16)).reshape(
        CAP, EXPERTS, D
    )
    arrived = lax.all_to_all(outgoing, ("ep", "tp"), split_axis=1, concat_axis=1, tiled=True)
    local_count = expert_gate.shape[0]
    grouped = arrived.reshape(CAP, -1, local_count, D)
    gate_values = jnp.einsum(
        "csed,edf->csef", grouped, expert_gate, preferred_element_type=jnp.float32
    )
    upward = jnp.einsum("csed,edf->csef", grouped, expert_up, preferred_element_type=jnp.float32)
    hidden = (jax.nn.silu(gate_values) * upward).astype(jnp.bfloat16)
    produced = (
        jnp.einsum("csef,efd->csed", hidden, expert_down, preferred_element_type=jnp.float32)
        .astype(jnp.bfloat16)
        .reshape(CAP, -1, D)
    )
    returned = lax.all_to_all(produced, ("ep", "tp"), split_axis=1, concat_axis=1, tiled=True)
    picked_rows = returned.reshape(CAP * EXPERTS, D)[slot_index].reshape(row_count, TOP_K, D)
    routed = jnp.sum(route_weights[:, :, None] * picked_rows.astype(jnp.float32), axis=1)
    return (shared_out.astype(jnp.float32) + routed).astype(jnp.bfloat16)


def local(
    queries,
    key_vectors,
    values,
    forget_cum,
    query_gain,
    key_gain,
    tokens,
    norm_gain,
    routes,
    route_weights,
    expert_gate,
    expert_up,
    expert_down,
    shared_gate,
    shared_up,
    shared_down,
):
    attended = attend(queries, key_vectors, values, forget_cum, query_gain, key_gain)
    routed_output = mixture(
        tokens,
        norm_gain,
        routes,
        route_weights,
        expert_gate,
        expert_up,
        expert_down,
        shared_gate,
        shared_up,
        shared_down,
    )
    return (attended, routed_output)


def rms_heads(wide, gain, heads):
    pieces = []
    for h in range(heads):
        part = wide[:, h, :]
        inverse = lax.rsqrt(jnp.mean(part * part, axis=-1, keepdims=True) + 1e-06)
        pieces.append((part * inverse * gain).astype(BF16))
    return jnp.concatenate(pieces, axis=1)


def iota(shape, axis):
    return lax.broadcasted_iota(jnp.int32, shape, axis)


def fused_kernel(
    n_ep,
    n_tp,
    heads,
    tokens_ref,
    gain_ref,
    routes_ref,
    weights_ref,
    q_ref,
    k_ref,
    v_ref,
    qg_ref,
    kg_ref,
    cum_ref,
    gate_ref,
    up_ref,
    down_ref,
    sg_ref,
    su_ref,
    sd_ref,
    att_ref,
    res_ref,
    tok,
    gain,
    routes,
    weights,
    q_in,
    k_in,
    v_in,
    q_gain,
    k_gain,
    cum,
    normed,
    pick,
    comb,
    gather,
    scatter,
    outgoing,
    x_buf,
    x_rows,
    wide_w,
    down_w,
    y_rows,
    y_buf,
    r_buf,
    sh_buf,
    total,
    qn,
    kv_buf,
    q_far,
    far_out,
    far_in,
    stat_out,
    stat_in,
    in_sem,
    w_sem,
    x_send,
    x_recv,
    x_own,
    y_send,
    y_recv,
    y_own,
    sh_send,
    sh_recv,
    sh_own,
    sf_send,
    sf_recv,
    kv_send,
    kv_recv,
    q_send,
    q_recv,
    far_send,
    far_recv,
    out_sem,
):
    e_pos = lax.axis_index("ep")
    t_pos = lax.axis_index("tp")
    count = n_ep * n_tp
    me = e_pos * n_tp + t_pos
    local_count = gate_ref.shape[0]
    per = local_count // GROUPS
    hidden_width = gate_ref.shape[2]
    block = HALVES * per * CAP
    slots = count * block
    expert_rows = count * CAP
    group_rows = per * expert_rows
    rows, dim = tok.shape
    half = dim // HALVES
    x_wide = half // SENDS
    y_wide = half // RETURNS
    peer_rows = (count - 1) * block

    def device(i):
        return {"ep": i // n_tp, "tp": i % n_tp}

    barrier = pltpu.get_barrier_semaphore()

    def greet(i, carry):
        pl.semaphore_signal(
            barrier, inc=1, device_id=device((me + i) % count), device_id_type=MESH
        )
        return carry

    lax.fori_loop(1, count, greet, 0)
    inputs = [
        pltpu.make_async_copy(src, dst, in_sem.at[i])
        for i, (src, dst) in enumerate(
            (
                (routes_ref, routes),
                (tokens_ref, tok),
                (gain_ref, gain),
                (weights_ref, weights),
                (k_ref, k_in),
                (v_ref, v_in),
                (q_ref, q_in),
                (qg_ref, q_gain),
                (kg_ref, k_gain),
                (cum_ref, cum),
            )
        )
    ]
    for copy in inputs:
        copy.start()

    def weight_copies(g, e):
        n = g * per + e
        return (
            pltpu.make_async_copy(
                gate_ref.at[n], wide_w.at[e, :, pl.ds(0, hidden_width)], w_sem.at[e, 0]
            ),
            pltpu.make_async_copy(
                up_ref.at[n], wide_w.at[e, :, pl.ds(hidden_width, hidden_width)], w_sem.at[e, 1]
            ),
            pltpu.make_async_copy(down_ref.at[n], down_w.at[e], w_sem.at[e, 2]),
        )

    def first_weights(e, carry):
        for copy in weight_copies(0, e):
            copy.start()
        return carry

    shared_refs = (sg_ref, su_ref, sd_ref)
    part = sd_ref.shape[0]
    own_shared = [
        pltpu.make_async_copy(src, sh_buf.at[t_pos, pl.ds(j * part, part)], sh_own.at[j])
        for j, src in enumerate(shared_refs)
    ]

    inputs[0].wait()
    inputs[3].wait()
    lax.fori_loop(0, per, first_weights, 0)
    for copy in own_shared:
        copy.start()

    r = iota((slots, rows), 0)
    which_half = (r % block) // (per * CAP)
    before = jnp.where(iota((rows, rows), 0) < iota((rows, rows), 1), 1.0, 0.0).astype(BF16)

    def chosen(g):
        expert = (r // block) * local_count + g * per + (r % (per * CAP)) // CAP
        first = expert == routes[0:1, :]
        named = jnp.where(first | (expert == routes[1:2, :]), 1.0, 0.0)
        earlier = jnp.dot(named.astype(BF16), before, preferred_element_type=F32)
        return first, jnp.where(earlier == (r % CAP).astype(F32), named, 0.0)

    def fill_pick(g):
        _, hit = chosen(g)
        for h in range(HALVES):
            pick[g, :, h * rows : (h + 1) * rows] = jnp.where(which_half == h, hit, 0.0).astype(
                BF16
            )

    fill_pick(0)
    inputs[1].wait()
    inputs[2].wait()
    wide = tok[...].astype(F32)
    inverse = lax.rsqrt(jnp.mean(wide * wide, axis=-1, keepdims=True) + 1e-06)
    step = half // 4
    for h in range(HALVES):
        for c in range(4):
            cols = slice(h * half + c * step, h * half + (c + 1) * step)
            normed[h * rows : (h + 1) * rows, c * step : (c + 1) * step] = (
                tok[:, cols].astype(F32) * inverse * gain[:, cols]
            ).astype(BF16)
    pl.semaphore_wait(barrier, count - 1)

    def rows_of(i):
        return pl.ds(pl.multiple_of(i * block, block), block)

    across_z = ((e_pos + 2) % n_ep, n_ep - 1 - e_pos, e_pos + 1 - 2 * (e_pos % 2), e_pos)

    def to_peers(src, dst, send_sem, recv_sem):
        for k, e in enumerate(across_z):

            def send(j, carry):
                peer = e * n_tp + (t_pos + j) % n_tp
                pltpu.make_async_remote_copy(
                    src_ref=src.at[rows_of(peer)],
                    dst_ref=dst.at[rows_of(me)],
                    send_sem=send_sem,
                    recv_sem=recv_sem,
                    device_id=device(peer),
                    device_id_type=MESH,
                ).start()
                return carry

            lax.fori_loop(1 if k == 3 else 0, n_tp, send, 0)

    def pick_rows(g, c):
        outgoing[g, c] = jnp.dot(
            pick[g], normed[:, c * x_wide : (c + 1) * x_wide], preferred_element_type=F32
        ).astype(BF16)

    def dispatch(g, c):
        pltpu.make_async_copy(
            outgoing.at[g, c, rows_of(me)], x_buf.at[g, c, rows_of(me)], x_own.at[g, c]
        ).start()
        to_peers(outgoing.at[g, c], x_buf.at[g, c], x_send.at[g], x_recv.at[g])

    mate = t_pos + 1 - 2 * (t_pos % 2)
    across = (t_pos + 2) % n_tp
    sh_wide = dim // SHARED

    def shared_send(c):
        cols = pl.ds(c * sh_wide, sh_wide)
        for s, target in enumerate((mate, across)):
            for j, src in enumerate(shared_refs):
                pltpu.make_async_remote_copy(
                    src_ref=src.at[:, cols],
                    dst_ref=sh_buf.at[t_pos, pl.ds(j * part, part), cols],
                    send_sem=sh_send.at[s, c],
                    recv_sem=sh_recv.at[s, c],
                    device_id={"tp": target},
                    device_id_type=MESH,
                ).start()

    pick_rows(0, 0)
    for c in range(1, SENDS):
        pick_rows(0, c)
        dispatch(0, c - 1)
    for g in range(1, GROUPS):
        fill_pick(g)
    dispatch(0, SENDS - 1)

    for copy in inputs[4:]:
        copy.wait()
    qn[...] = rms_heads(q_in[...].astype(F32), q_gain[...], heads)
    kv_buf[e_pos % 2, 0] = rms_heads(k_in[...].astype(F32), k_gain[...], heads)
    held = v_in[...].astype(F32)
    kv_buf[e_pos % 2, 1] = jnp.concatenate(
        [held[:, h, :].astype(BF16) for h in range(heads)], axis=1
    )

    @pl.when(e_pos % 2 == 0)
    def _():
        kv_buf[1] = jnp.zeros(kv_buf.shape[1:], BF16)

    for g in range(1, GROUPS):
        for c in range(SENDS):
            pick_rows(g, c)

    def kv_copy(j):
        return pltpu.make_async_remote_copy(
            src_ref=kv_buf.at[0, j],
            dst_ref=kv_buf.at[0, j],
            send_sem=kv_send.at[j],
            recv_sem=kv_recv.at[j],
            device_id={"ep": jnp.minimum(e_pos + 1, n_ep - 1)},
            device_id_type=MESH,
        )

    far_index = jnp.maximum(e_pos - 2, 0)

    def q_copy():
        return pltpu.make_async_remote_copy(
            src_ref=qn,
            dst_ref=q_far.at[far_index],
            send_sem=q_send,
            recv_sem=q_recv.at[far_index],
            device_id={"ep": 1},
            device_id_type=MESH,
        )

    @pl.when(e_pos % 2 == 0)
    def _():
        for j in range(2):
            kv_copy(j).start()

    @pl.when(e_pos >= 2)
    def _():
        q_copy().start()

    for g in range(1, GROUPS):
        for c in range(SENDS):
            dispatch(g, c)
    shared_send(0)

    big_row = iota((slots, HALVES * group_rows), 1)
    big_slot = iota((slots, HALVES * group_rows), 0)

    def slot_of(n):
        h = n // group_rows
        e = (n % group_rows) // expert_rows
        src = (n % expert_rows) // CAP
        return src * block + h * (per * CAP) + e * CAP + n % CAP

    scatter[...] = jnp.where(slot_of(big_row) == big_slot, 1.0, 0.0).astype(BF16)
    big_row = iota((HALVES * group_rows, slots), 0)
    big_slot = iota((HALVES * group_rows, slots), 1)
    gather[...] = jnp.where(slot_of(big_row) == big_slot, 1.0, 0.0).astype(BF16)

    for g in range(GROUPS):
        first, hit = chosen(g)
        weight = jnp.where(first, weights[0:1, :], weights[1:2, :]) * hit
        for h in range(HALVES):
            mine = jnp.where(which_half == h, weight, 0.0).T
            high = mine.astype(BF16)
            comb[g, h] = high
            comb[g, HALVES + h] = (mine - high.astype(F32)).astype(BF16)

    size = qn.shape[1] // heads
    contract = (((1,), (1,)), ((), ()))
    diagonal = iota((rows, rows), 0) == iota((rows, rows), 1)

    def column(row):
        return jnp.sum(jnp.where(diagonal, row, 0.0), axis=1, keepdims=True)

    def as_row(col):
        return jnp.sum(jnp.where(diagonal, col, 0.0), axis=0, keepdims=True)

    def span_of(h):
        return slice(h * size, (h + 1) * size)

    def attend_pair(h, q, query_start, key_start, allowed):
        query_span = pl.ds(pl.multiple_of(query_start, rows), rows)
        key_span = pl.ds(pl.multiple_of(key_start, 2 * rows), 2 * rows)
        scores = jnp.concatenate(
            [
                lax.dot_general(
                    q, kv_buf[b, 0, :, span_of(h)], contract, preferred_element_type=F32
                )
                for b in range(2)
            ],
            axis=1,
        )
        scores = (
            scores * (size**-0.5)
            + column(cum[h : h + 1, query_span])
            - cum[h : h + 1, key_span]
        )
        if allowed is not None:
            scores = jnp.where(allowed, scores, -1e30)
        top = jnp.max(scores, axis=1, keepdims=True)
        probs = jnp.exp(scores - top)
        if allowed is not None:
            probs = jnp.where(allowed, probs, 0.0)
        norm = jnp.sum(probs, axis=1, keepdims=True)
        probs = probs.astype(BF16)
        mixed = jnp.dot(
            probs[:, :rows], kv_buf[0, 1, :, span_of(h)], preferred_element_type=F32
        ) + jnp.dot(probs[:, rows:], kv_buf[1, 1, :, span_of(h)], preferred_element_type=F32)
        return top, norm, mixed

    def compute(g):
        pltpu.make_async_copy(
            x_buf.at[g, :, pl.ds(0, peer_rows)],
            x_buf.at[g, :, pl.ds(0, peer_rows)],
            x_recv.at[g],
        ).wait()
        for c in range(SENDS):
            pltpu.make_async_copy(
                x_buf.at[g, c, pl.ds(0, block)], x_buf.at[g, c, pl.ds(0, block)], x_own.at[g, c]
            ).wait()
        for c in range(SENDS):
            ordered = jnp.dot(gather[...], x_buf[g, c], preferred_element_type=F32).astype(BF16)
            for h in range(HALVES):
                start = h * half + c * x_wide
                x_rows[:, start : start + x_wide] = ordered[
                    h * group_rows : (h + 1) * group_rows
                ]

        def one(e, carry):
            copies = weight_copies(g, e)
            span = pl.ds(pl.multiple_of(e * expert_rows, expert_rows), expert_rows)
            copies[0].wait()
            copies[1].wait()
            both = jnp.dot(x_rows[span], wide_w[e], preferred_element_type=F32)
            gate = both[:, :hidden_width]
            hidden = (gate / (1.0 + jnp.exp(-gate)) * both[:, hidden_width:]).astype(BF16)
            copies[2].wait()
            for h in range(HALVES):
                at = pl.ds(pl.multiple_of(h * group_rows + e * expert_rows, expert_rows), expert_rows)
                for c in range(2):
                    cols = slice(c * half // 2, (c + 1) * half // 2)
                    y_rows[at, cols] = jnp.dot(
                        hidden,
                        down_w[e, :, h * half + c * half // 2 : h * half + (c + 1) * half // 2],
                        preferred_element_type=F32,
                    ).astype(BF16)
            if g + 1 < GROUPS:
                for copy in weight_copies(g + 1, e):
                    copy.start()
            return carry

        lax.fori_loop(0, per, one, 0)

    def place(g, c):
        y_buf[g, c] = jnp.dot(
            scatter[...], y_rows[:, c * y_wide : (c + 1) * y_wide], preferred_element_type=F32
        ).astype(BF16)

    def give(g, c):
        pltpu.make_async_copy(
            y_buf.at[g, c, rows_of(me)], r_buf.at[g, c, rows_of(me)], y_own.at[g, c]
        ).start()
        to_peers(y_buf.at[g, c], r_buf.at[g, c], y_send.at[g], y_recv.at[g, c])

    def give_back(g):
        place(g, 0)
        for c in range(1, RETURNS):
            place(g, c)
            give(g, c - 1)

    compute(0)
    give_back(0)
    shared_send(1)

    @pl.when(e_pos % 2 == 1)
    def _():
        for j in range(2):
            kv_copy(j).wait_recv()

    give(0, RETURNS - 1)

    @pl.when(e_pos == 1)
    def _():
        for i in range(2):
            pltpu.make_async_copy(q_far.at[i], q_far.at[i], q_recv.at[i]).wait()
            for h in range(heads):
                top, norm, mixed = attend_pair(
                    h, q_far[i, :, span_of(h)], (2 + i) * rows, 0, None
                )
                far_out[i, :, span_of(h)] = mixed.astype(BF16)
                stat_out[i, h : h + 1] = as_row(top)
                stat_out[i, heads + h : heads + h + 1] = as_row(norm)

    at = (e_pos % 2) * rows + iota((rows, 2 * rows), 0)
    allowed = iota((rows, 2 * rows), 1) <= at
    near = [
        attend_pair(h, qn[:, span_of(h)], e_pos * rows, (e_pos // 2) * 2 * rows, allowed)
        for h in range(heads)
    ]
    for h in range(heads):
        total[:, span_of(h)] = near[h][2]

    def far_copies(i):
        return (
            pltpu.make_async_remote_copy(
                src_ref=far_out.at[i],
                dst_ref=far_in,
                send_sem=far_send.at[i, 0],
                recv_sem=far_recv.at[0],
                device_id={"ep": 2 + i},
                device_id_type=MESH,
            ),
            pltpu.make_async_remote_copy(
                src_ref=stat_out.at[i],
                dst_ref=stat_in,
                send_sem=far_send.at[i, 1],
                recv_sem=far_recv.at[1],
                device_id={"ep": 2 + i},
                device_id_type=MESH,
            ),
        )

    @pl.when(e_pos == 1)
    def _():
        for i in range(2):
            for copy in far_copies(i):
                copy.start()

    shared_send(2)
    compute(1)
    give_back(1)
    shared_send(3)

    @pl.when(e_pos < 2)
    def _():
        far_in[...] = jnp.zeros(far_in.shape, BF16)
        stat_in[0:heads] = jnp.full((heads, rows), -1e30, F32)
        stat_in[heads:] = jnp.zeros((stat_in.shape[0] - heads, rows), F32)

    give(1, RETURNS - 1)

    @pl.when(e_pos >= 2)
    def _():
        for copy in far_copies(0):
            copy.wait_recv()

    parts = []
    for h in range(heads):
        top, norm, _ = near[h]
        far_top = column(stat_in[h : h + 1])
        best = jnp.maximum(top, far_top)
        near_scale = jnp.exp(top - best)
        far_scale = jnp.exp(far_top - best)
        far_norm = column(stat_in[heads + h : heads + h + 1])
        mixed = total[:, span_of(h)] * near_scale + far_in[:, span_of(h)].astype(F32) * far_scale
        parts.append(mixed / (norm * near_scale + far_norm * far_scale))
    att_ref[...] = jnp.stack(parts, axis=1).astype(BF16)

    across_copies = []
    for c in range(SHARED):
        cols = pl.ds(c * sh_wide, sh_wide)
        pltpu.make_async_copy(
            sh_buf.at[across, :, cols], sh_buf.at[across, :, cols], sh_recv.at[1, c]
        ).wait()
        copy = pltpu.make_async_remote_copy(
            src_ref=sh_buf.at[across, :, cols],
            dst_ref=sh_buf.at[across, :, cols],
            send_sem=sf_send.at[c],
            recv_sem=sf_recv.at[c],
            device_id={"tp": mate},
            device_id_type=MESH,
        )
        copy.start()
        across_copies.append(copy)
    for copy in own_shared:
        copy.wait()
    third = mate + 2 - 4 * (mate // 2)
    for c in range(SHARED):
        cols = pl.ds(c * sh_wide, sh_wide)
        pltpu.make_async_copy(
            sh_buf.at[mate, :, cols], sh_buf.at[mate, :, cols], sh_recv.at[0, c]
        ).wait()
        pltpu.make_async_copy(
            sh_buf.at[third, :, cols], sh_buf.at[third, :, cols], sf_recv.at[c]
        ).wait()
    hidden_parts = []
    for blk in range(n_tp):
        both = [
            sum(
                lax.dot_general(
                    normed[h * rows : (h + 1) * rows, :],
                    sh_buf[blk, j * part : (j + 1) * part, h * half : (h + 1) * half],
                    contract,
                    preferred_element_type=F32,
                )
                for h in range(HALVES)
            )
            for j in range(2)
        ]
        hidden_parts.append((both[0] / (1.0 + jnp.exp(-both[0])) * both[1]).astype(BF16))
    narrow = dim // 8
    for c in range(8):
        cols = slice(c * narrow, (c + 1) * narrow)
        summed = jnp.zeros((rows, narrow), F32)
        for blk in range(n_tp):
            piece = jnp.dot(
                hidden_parts[blk],
                sh_buf[blk, 2 * part : 3 * part, cols],
                preferred_element_type=F32,
            )
            summed += piece.astype(BF16).astype(F32)
        total[:, cols] = summed.astype(BF16).astype(F32)

    def returned(g, c):
        pltpu.make_async_copy(
            r_buf.at[g, c, pl.ds(0, peer_rows)],
            r_buf.at[g, c, pl.ds(0, peer_rows)],
            y_recv.at[g, c],
        ).wait()
        pltpu.make_async_copy(
            r_buf.at[g, c, pl.ds(0, block)], r_buf.at[g, c, pl.ds(0, block)], y_own.at[g, c]
        ).wait()
        back = r_buf[g, c]
        for h in range(HALVES):
            cols = slice(h * half + c * y_wide, h * half + (c + 1) * y_wide)
            routed = jnp.dot(comb[g, h], back, preferred_element_type=F32) + jnp.dot(
                comb[g, HALVES + h], back, preferred_element_type=F32
            )
            if g + 1 < GROUPS:
                total[:, cols] += routed
            else:
                tok[:, cols] = (total[:, cols] + routed).astype(BF16)

    for g in range(GROUPS - 1):
        for c in range(RETURNS):
            returned(g, c)
    outs = []
    for c in range(RETURNS):
        returned(GROUPS - 1, c)
        for h in range(HALVES):
            cols = pl.ds(h * half + c * y_wide, y_wide)
            copy = pltpu.make_async_copy(tok.at[:, cols], res_ref.at[:, cols], out_sem.at[c, h])
            copy.start()
            outs.append(copy)

    for g in range(GROUPS):
        pltpu.make_async_copy(
            x_buf.at[g, :, pl.ds(0, peer_rows)],
            x_buf.at[g, :, pl.ds(0, peer_rows)],
            x_send.at[g],
        ).wait()
        pltpu.make_async_copy(
            y_buf.at[g, :, pl.ds(0, peer_rows)],
            y_buf.at[g, :, pl.ds(0, peer_rows)],
            y_send.at[g],
        ).wait()
    for c in range(SHARED):
        cols = pl.ds(c * sh_wide, sh_wide)
        for s in range(2):
            pltpu.make_async_copy(
                sh_buf.at[t_pos, :, cols], sh_buf.at[t_pos, :, cols], sh_send.at[s, c]
            ).wait()
        across_copies[c].wait_send()

    @pl.when(e_pos % 2 == 0)
    def _():
        for j in range(2):
            kv_copy(j).wait_send()

    @pl.when(e_pos >= 2)
    def _():
        q_copy().wait_send()

    @pl.when(e_pos == 1)
    def _():
        for i in range(2):
            for copy in far_copies(i):
                copy.wait_send()

    for copy in outs:
        copy.wait()


def fused_local(n_ep, n_tp, *args):
    (
        queries,
        key_vectors,
        values,
        forget_cum,
        query_gain,
        key_gain,
        tokens,
        norm_gain,
        routes,
        route_weights,
        expert_gate,
        expert_up,
        expert_down,
        shared_gate,
        shared_up,
        shared_down,
    ) = args
    rows, heads, size = queries.shape
    row_count, dim = tokens.shape
    local_count, _, hidden = expert_gate.shape
    count = n_ep * n_tp
    per = local_count // GROUPS
    slots = count * HALVES * per * CAP
    group_rows = count * per * CAP
    half = dim // HALVES
    part = shared_gate.shape[1]
    flat = heads * size
    hbm = pl.BlockSpec(memory_space=pltpu.HBM)
    sds = jax.ShapeDtypeStruct
    vmem = pltpu.VMEM
    dma = pltpu.SemaphoreType.DMA
    attended, routed = pl.pallas_call(
        functools.partial(fused_kernel, n_ep, n_tp, heads),
        out_shape=(sds((rows, heads, size), BF16), sds((row_count, dim), BF16)),
        in_specs=[hbm] * 16,
        out_specs=[pl.BlockSpec(memory_space=pltpu.VMEM), hbm],
        scratch_shapes=[
            vmem((row_count, dim), BF16),
            vmem((1, dim), F32),
            vmem((TOP_K, row_count), jnp.int32),
            vmem((TOP_K, row_count), F32),
            vmem((rows, heads, size), BF16),
            vmem((rows, heads, size), BF16),
            vmem((rows, heads, size), BF16),
            vmem((1, size), F32),
            vmem((1, size), F32),
            vmem((heads, n_ep * rows), F32),
            vmem((HALVES * row_count, half), BF16),
            vmem((GROUPS, slots, HALVES * row_count), BF16),
            vmem((GROUPS, 2 * HALVES, row_count, slots), BF16),
            vmem((HALVES * group_rows, slots), BF16),
            vmem((slots, HALVES * group_rows), BF16),
            vmem((GROUPS, SENDS, slots, half // SENDS), BF16),
            vmem((GROUPS, SENDS, slots, half // SENDS), BF16),
            vmem((group_rows, dim), BF16),
            vmem((per, dim, 2 * hidden), BF16),
            vmem((per, hidden, dim), BF16),
            vmem((HALVES * group_rows, half), BF16),
            vmem((GROUPS, RETURNS, slots, half // RETURNS), BF16),
            vmem((GROUPS, RETURNS, slots, half // RETURNS), BF16),
            vmem((n_tp, 3 * part, dim), BF16),
            vmem((row_count, dim), F32),
            vmem((rows, flat), BF16),
            vmem((2, 2, rows, flat), BF16),
            vmem((2, rows, flat), BF16),
            vmem((2, rows, flat), BF16),
            vmem((rows, flat), BF16),
            vmem((2, 2 * heads, rows), F32),
            vmem((2 * heads, rows), F32),
            dma((10,)),
            dma((per, 3)),
            dma((GROUPS,)),
            dma((GROUPS,)),
            dma((GROUPS, SENDS)),
            dma((GROUPS,)),
            dma((GROUPS, RETURNS)),
            dma((GROUPS, RETURNS)),
            dma((2, SHARED)),
            dma((2, SHARED)),
            dma((3,)),
            dma((SHARED,)),
            dma((SHARED,)),
            dma((2,)),
            dma((2,)),
            dma,
            dma((2,)),
            dma((2, 2)),
            dma((2,)),
            dma((RETURNS, HALVES)),
        ],
        compiler_params=pltpu.CompilerParams(
            collective_id=0, has_side_effects=True, vmem_limit_bytes=60 * 1024 * 1024
        ),
        name="fused",
    )(
        tokens,
        norm_gain.reshape(1, dim),
        routes.T,
        route_weights.T,
        queries,
        key_vectors,
        values,
        query_gain.reshape(1, size),
        key_gain.reshape(1, size),
        forget_cum.T,
        expert_gate,
        expert_up,
        expert_down,
        shared_gate.T,
        shared_up.T,
        shared_down,
    )
    return attended, routed


def local_of(mesh):
    n_ep, n_tp = mesh.shape["ep"], mesh.shape["tp"]

    def run(*args):
        experts = args[10]
        block = CAP * experts.shape[0]
        if n_tp == 4 and n_ep == 4 and block % 16 == 0 and args[15].shape[0] % 16 == 0:
            return fused_local(n_ep, n_tp, *args)
        return local(*args)

    return run


def solution(mesh):
    placed = (
        P(("grp", "ep"), "tp", None),
        P(("grp", "ep"), "tp", None),
        P(("grp", "ep"), "tp", None),
        P("grp", "tp"),
        P(),
        P(),
        P(("grp", "ep", "tp"), None),
        P(),
        P(("grp", "ep", "tp"), None),
        P(("grp", "ep", "tp"), None),
        P(("ep", "tp"), None, None),
        P(("ep", "tp"), None, None),
        P(("ep", "tp"), None, None),
        P(None, "tp"),
        P(None, "tp"),
        P("tp", None),
    )
    return jax.shard_map(
        local_of(mesh),
        mesh=mesh,
        in_specs=placed,
        out_specs=(P(("grp", "ep"), "tp", None), P(("grp", "ep", "tp"), None)),
        check_vma=False,
    )
```

```python
import functools
import jax
import jax.numpy as jnp
from jax import lax
from jax.experimental import pallas as pl
from jax.experimental.pallas import tpu as pltpu
from jax.sharding import PartitionSpec as P

MESH = pl.DeviceIdType.MESH
F32 = jnp.float32
BF16 = jnp.bfloat16
CAP = 2
GROUPS = 2
HALVES = 2
SENDS = 4
RETURNS = 4
SHARED = 4
AHEAD = 3

D = 4096
EXPERTS = 128
TOP_K = 2


def rms_rows(row_values, gain_vector):
    widened = row_values.astype(jnp.float32)
    inverse = lax.rsqrt(jnp.mean(widened * widened, axis=-1, keepdims=True) + 1e-06)
    return (widened * inverse * gain_vector).astype(jnp.bfloat16)


def attend(queries, key_vectors, values, forget_cum, query_gain, key_gain):
    query_norm = rms_rows(queries, query_gain)
    key_norm = rms_rows(key_vectors, key_gain)
    query_rows = query_norm.shape[0]
    head_count = query_norm.shape[1]
    head_size = query_norm.shape[2]
    first_query = lax.axis_index("ep") * query_rows
    query_positions = first_query + lax.iota(jnp.int32, query_rows)
    last_query = first_query + query_rows - 1
    query_cum = lax.dynamic_slice_in_dim(forget_cum, first_query, query_rows, 0).T
    scale_factor = head_size ** (-0.5)
    start_state = (
        jnp.full((head_count, query_rows), -1e30, jnp.float32),
        jnp.zeros((head_count, query_rows), jnp.float32),
        jnp.zeros((head_count, query_rows, head_size), jnp.float32),
    )
    key_part = lax.all_gather(key_norm, "ep", axis=0, tiled=True)
    value_part = lax.all_gather(values, "ep", axis=0, tiled=True)
    piece_rows = key_part.shape[0]

    def compute(inner_state):
        best_score, denominator, accumulated = inner_state
        cum_block = forget_cum.T
        scores = jnp.einsum(
            "qhd,khd->hqk", query_norm, key_part, preferred_element_type=jnp.float32
        )
        scores = scores * scale_factor + query_cum[:, :, None] - cum_block[:, None, :]
        key_positions = lax.iota(jnp.int32, piece_rows)
        allowed = (key_positions[None, :] <= query_positions[:, None])[None]
        scores = jnp.where(allowed, scores, -1e30)
        new_best = jnp.maximum(best_score, jnp.max(scores, axis=2))
        weights = jnp.where(allowed, jnp.exp(scores - new_best[:, :, None]), 0.0)
        denominator = jnp.sum(weights, axis=2)
        product = jnp.einsum(
            "hqk,khd->hqd",
            weights.astype(jnp.bfloat16),
            value_part,
            preferred_element_type=jnp.float32,
        )
        accumulated = product
        return (new_best, denominator, accumulated)

    best_score, denominator, accumulated = lax.cond(
        jnp.int32(0) <= last_query, compute, lambda inner_state: inner_state, start_state
    )
    return (accumulated / denominator[:, :, None]).transpose(1, 0, 2).astype(jnp.bfloat16)


def shared_expert(normed, shared_gate, shared_up, shared_down):
    row_count = normed.shape[0]
    whole_gate, whole_up, whole_down = (
        lax.all_gather(shared_gate, "tp", axis=1, tiled=True),
        lax.all_gather(shared_up, "tp", axis=1, tiled=True),
        lax.all_gather(shared_down, "tp", axis=0, tiled=True),
    )
    block_total = lax.axis_size("tp")
    gate_values = jnp.dot(normed, whole_gate, preferred_element_type=jnp.float32)
    upward = jnp.dot(normed, whole_up, preferred_element_type=jnp.float32)
    hidden_whole = (jax.nn.silu(gate_values) * upward).astype(jnp.bfloat16)
    part_width = whole_down.shape[0] // block_total
    hidden_blocks = hidden_whole.reshape(row_count, block_total, part_width)
    down_blocks = whole_down.reshape(block_total, part_width, whole_down.shape[1])
    partials = jnp.einsum(
        "rnp,npd->nrd", hidden_blocks, down_blocks, preferred_element_type=jnp.float32
    ).astype(jnp.bfloat16)
    return jnp.sum(partials.astype(jnp.float32), axis=0).astype(jnp.bfloat16)


def mixture(
    tokens,
    norm_gain,
    routes,
    route_weights,
    expert_gate,
    expert_up,
    expert_down,
    shared_gate,
    shared_up,
    shared_down,
):
    normed = rms_rows(tokens, norm_gain)
    row_count = tokens.shape[0]
    shared_out = shared_expert(normed, shared_gate, shared_up, shared_down)
    flat_routes = routes.reshape(-1)
    choice_count = flat_routes.shape[0]
    one_hot = (flat_routes[:, None] == lax.iota(jnp.int32, EXPERTS)[None, :]).astype(jnp.int32)
    slot_rank = jnp.sum((jnp.cumsum(one_hot, axis=0) - one_hot) * one_hot, axis=1)
    slot_index = slot_rank * EXPERTS + flat_routes
    slot_ids = lax.iota(jnp.int32, CAP * EXPERTS)
    matches = slot_index[None, :] == slot_ids[:, None]
    source_row = jnp.sum(
        jnp.where(matches, lax.iota(jnp.int32, choice_count)[None, :] // TOP_K, 0), axis=1
    )
    filled = jnp.any(matches, axis=1)
    outgoing = jnp.where(filled[:, None], normed[source_row], jnp.zeros((), jnp.bfloat16)).reshape(
        CAP, EXPERTS, D
    )
    arrived = lax.all_to_all(outgoing, ("ep", "tp"), split_axis=1, concat_axis=1, tiled=True)
    local_count = expert_gate.shape[0]
    grouped = arrived.reshape(CAP, -1, local_count, D)
    gate_values = jnp.einsum(
        "csed,edf->csef", grouped, expert_gate, preferred_element_type=jnp.float32
    )
    upward = jnp.einsum("csed,edf->csef", grouped, expert_up, preferred_element_type=jnp.float32)
    hidden = (jax.nn.silu(gate_values) * upward).astype(jnp.bfloat16)
    produced = (
        jnp.einsum("csef,efd->csed", hidden, expert_down, preferred_element_type=jnp.float32)
        .astype(jnp.bfloat16)
        .reshape(CAP, -1, D)
    )
    returned = lax.all_to_all(produced, ("ep", "tp"), split_axis=1, concat_axis=1, tiled=True)
    picked_rows = returned.reshape(CAP * EXPERTS, D)[slot_index].reshape(row_count, TOP_K, D)
    routed = jnp.sum(route_weights[:, :, None] * picked_rows.astype(jnp.float32), axis=1)
    return (shared_out.astype(jnp.float32) + routed).astype(jnp.bfloat16)


def local(
    queries,
    key_vectors,
    values,
    forget_cum,
    query_gain,
    key_gain,
    tokens,
    norm_gain,
    routes,
    route_weights,
    expert_gate,
    expert_up,
    expert_down,
    shared_gate,
    shared_up,
    shared_down,
):
    attended = attend(queries, key_vectors, values, forget_cum, query_gain, key_gain)
    routed_output = mixture(
        tokens,
        norm_gain,
        routes,
        route_weights,
        expert_gate,
        expert_up,
        expert_down,
        shared_gate,
        shared_up,
        shared_down,
    )
    return (attended, routed_output)


def rms_heads(wide, gain, heads):
    pieces = []
    for h in range(heads):
        part = wide[:, h, :]
        inverse = lax.rsqrt(jnp.mean(part * part, axis=-1, keepdims=True) + 1e-06)
        pieces.append((part * inverse * gain).astype(BF16))
    return jnp.concatenate(pieces, axis=1)


def iota(shape, axis):
    return lax.broadcasted_iota(jnp.int32, shape, axis)


def fused_kernel(
    n_ep,
    n_tp,
    heads,
    tokens_ref,
    gain_ref,
    routes_ref,
    weights_ref,
    q_ref,
    k_ref,
    v_ref,
    qg_ref,
    kg_ref,
    cum_ref,
    gate_ref,
    up_ref,
    down_ref,
    sg_ref,
    su_ref,
    sd_ref,
    att_ref,
    res_ref,
    tok,
    gain,
    routes,
    weights,
    q_in,
    k_in,
    v_in,
    q_gain,
    k_gain,
    cum,
    normed,
    pick,
    comb,
    gather,
    scatter,
    outgoing,
    x_buf,
    x_rows,
    wide_w,
    down_w,
    y_rows,
    y_buf,
    r_buf,
    sh_buf,
    total,
    qn,
    kv_buf,
    q_far,
    far_out,
    far_in,
    stat_out,
    stat_in,
    near_sum,
    in_sem,
    w_sem,
    x_send,
    x_recv,
    x_own,
    y_send,
    y_recv,
    y_own,
    sh_send,
    sh_recv,
    sh_own,
    sf_send,
    sf_recv,
    kv_send,
    kv_recv,
    q_send,
    q_recv,
    far_send,
    far_recv,
    credit,
):
    e_pos = lax.axis_index("ep")
    t_pos = lax.axis_index("tp")
    count = n_ep * n_tp
    me = e_pos * n_tp + t_pos
    local_count = gate_ref.shape[0]
    per = local_count // GROUPS
    hidden_width = gate_ref.shape[2]
    block = HALVES * per * CAP
    slots = count * block
    expert_rows = count * CAP
    group_rows = per * expert_rows
    rows, dim = tok.shape
    half = dim // HALVES
    x_wide = half // SENDS
    y_wide = half // RETURNS
    peer_rows = (count - 1) * block

    def device(i):
        return {"ep": i // n_tp, "tp": i % n_tp}

    barrier = pltpu.get_barrier_semaphore()

    def greet(i, carry):
        pl.semaphore_signal(
            barrier, inc=1, device_id=device((me + i) % count), device_id_type=MESH
        )
        return carry

    lax.fori_loop(1, count, greet, 0)
    inputs = [
        pltpu.make_async_copy(src, dst, in_sem.at[i])
        for i, (src, dst) in enumerate(
            (
                (routes_ref, routes),
                (tokens_ref, tok),
                (gain_ref, gain),
                (weights_ref, weights),
                (k_ref, k_in),
                (v_ref, v_in),
                (q_ref, q_in),
                (qg_ref, q_gain),
                (kg_ref, k_gain),
                (cum_ref, cum),
            )
        )
    ]
    for copy in inputs:
        copy.start()

    def weight_copies(g, e):
        n = g * per + e
        return (
            pltpu.make_async_copy(
                gate_ref.at[n], wide_w.at[e, :, pl.ds(0, hidden_width)], w_sem.at[e, 0]
            ),
            pltpu.make_async_copy(
                up_ref.at[n], wide_w.at[e, :, pl.ds(hidden_width, hidden_width)], w_sem.at[e, 1]
            ),
            pltpu.make_async_copy(down_ref.at[n], down_w.at[e], w_sem.at[e, 2]),
        )

    def first_weights(e, carry):
        for copy in weight_copies(0, e):
            copy.start()
        return carry

    shared_refs = (sg_ref, su_ref, sd_ref)
    part = sd_ref.shape[0]
    own_shared = [
        pltpu.make_async_copy(src, sh_buf.at[t_pos, pl.ds(j * part, part)], sh_own.at[j])
        for j, src in enumerate(shared_refs)
    ]

    inputs[0].wait()
    inputs[3].wait()
    lax.fori_loop(0, per, first_weights, 0)
    for copy in own_shared:
        copy.start()

    r = iota((slots, rows), 0)
    which_half = (r % block) // (per * CAP)
    before = jnp.where(iota((rows, rows), 0) < iota((rows, rows), 1), 1.0, 0.0).astype(BF16)

    def chosen(g):
        expert = (r // block) * local_count + g * per + (r % (per * CAP)) // CAP
        first = expert == routes[0:1, :]
        named = jnp.where(first | (expert == routes[1:2, :]), 1.0, 0.0)
        earlier = jnp.dot(named.astype(BF16), before, preferred_element_type=F32)
        return first, jnp.where(earlier == (r % CAP).astype(F32), named, 0.0)

    def fill_pick(g):
        _, hit = chosen(g)
        for h in range(HALVES):
            pick[g, :, h * rows : (h + 1) * rows] = jnp.where(which_half == h, hit, 0.0).astype(
                BF16
            )

    fill_pick(0)
    inputs[1].wait()
    inputs[2].wait()
    wide = tok[...].astype(F32)
    inverse = lax.rsqrt(jnp.mean(wide * wide, axis=-1, keepdims=True) + 1e-06)
    step = half // 4
    for h in range(HALVES):
        for c in range(4):
            cols = slice(h * half + c * step, h * half + (c + 1) * step)
            normed[h * rows : (h + 1) * rows, c * step : (c + 1) * step] = (
                tok[:, cols].astype(F32) * inverse * gain[:, cols]
            ).astype(BF16)
    pl.semaphore_wait(barrier, count - 1)

    def rows_of(i):
        return pl.ds(pl.multiple_of(i * block, block), block)

    across_z = ((e_pos + 2) % n_ep, n_ep - 1 - e_pos, e_pos + 1 - 2 * (e_pos % 2), e_pos)

    def to_peers(src, dst, send_sem, recv_sem):
        for k, e in enumerate(across_z):

            def send(j, carry):
                peer = e * n_tp + (t_pos + j) % n_tp
                pltpu.make_async_remote_copy(
                    src_ref=src.at[rows_of(peer)],
                    dst_ref=dst.at[rows_of(me)],
                    send_sem=send_sem,
                    recv_sem=recv_sem,
                    device_id=device(peer),
                    device_id_type=MESH,
                ).start()
                return carry

            lax.fori_loop(1 if k == 3 else 0, n_tp, send, 0)

    def pick_rows(g, c):
        outgoing[g, c] = jnp.dot(
            pick[g], normed[:, c * x_wide : (c + 1) * x_wide], preferred_element_type=F32
        ).astype(BF16)

    def dispatch(g, c):
        pltpu.make_async_copy(
            outgoing.at[g, c, rows_of(me)], x_buf.at[g, c, rows_of(me)], x_own.at[g, c]
        ).start()
        to_peers(outgoing.at[g, c], x_buf.at[g, c], x_send.at[g, c], x_recv.at[g, c])

    mate = t_pos + 1 - 2 * (t_pos % 2)
    across = (t_pos + 2) % n_tp
    sh_wide = dim // SHARED

    def shared_send(c):
        cols = pl.ds(c * sh_wide, sh_wide)
        for s, target in enumerate((mate, across)):
            for j, src in enumerate(shared_refs):
                pltpu.make_async_remote_copy(
                    src_ref=src.at[:, cols],
                    dst_ref=sh_buf.at[t_pos, pl.ds(j * part, part), cols],
                    send_sem=sh_send.at[s, c],
                    recv_sem=sh_recv.at[s, c],
                    device_id={"tp": target},
                    device_id_type=MESH,
                ).start()

    order = [(g, c) for g in range(GROUPS) for c in range(SENDS)]

    def arrived(n):
        g, c = order[n]
        pltpu.make_async_copy(
            x_buf.at[g, c, pl.ds(0, peer_rows)],
            x_buf.at[g, c, pl.ds(0, peer_rows)],
            x_recv.at[g, c],
        ).wait()
        pltpu.make_async_copy(
            x_buf.at[g, c, pl.ds(0, block)], x_buf.at[g, c, pl.ds(0, block)], x_own.at[g, c]
        ).wait()

    def sent(g, c):
        pltpu.make_async_copy(
            x_buf.at[g, c, pl.ds(0, peer_rows)],
            x_buf.at[g, c, pl.ds(0, peer_rows)],
            x_send.at[g, c],
        ).wait()

    pick_rows(*order[0])
    for n in range(1, AHEAD):
        pick_rows(*order[n])
        dispatch(*order[n - 1])
    for n in range(AHEAD, SENDS):
        pick_rows(*order[n])
    dispatch(*order[AHEAD - 1])
    for g in range(1, GROUPS):
        fill_pick(g)
    shared_send(0)

    for copy in inputs[4:]:
        copy.wait()
    qn[...] = rms_heads(q_in[...].astype(F32), q_gain[...], heads)
    kv_buf[e_pos % 2, 0] = rms_heads(k_in[...].astype(F32), k_gain[...], heads)
    held = v_in[...].astype(F32)
    kv_buf[e_pos % 2, 1] = jnp.concatenate(
        [held[:, h, :].astype(BF16) for h in range(heads)], axis=1
    )

    @pl.when(e_pos % 2 == 0)
    def _():
        kv_buf[1] = jnp.zeros(kv_buf.shape[1:], BF16)

    for g in range(1, GROUPS):
        for c in range(SENDS):
            pick_rows(g, c)

    def kv_copy(j):
        return pltpu.make_async_remote_copy(
            src_ref=kv_buf.at[0, j],
            dst_ref=kv_buf.at[0, j],
            send_sem=kv_send.at[j],
            recv_sem=kv_recv.at[j],
            device_id={"ep": jnp.minimum(e_pos + 1, n_ep - 1)},
            device_id_type=MESH,
        )

    far_index = jnp.maximum(e_pos - 2, 0)

    def q_copy():
        return pltpu.make_async_remote_copy(
            src_ref=qn,
            dst_ref=q_far.at[far_index],
            send_sem=q_send,
            recv_sem=q_recv.at[far_index],
            device_id={"ep": 1},
            device_id_type=MESH,
        )

    big_row = iota((slots, HALVES * group_rows), 1)
    big_slot = iota((slots, HALVES * group_rows), 0)

    def slot_of(n):
        h = n // group_rows
        e = (n % group_rows) // expert_rows
        src = (n % expert_rows) // CAP
        return src * block + h * (per * CAP) + e * CAP + n % CAP

    scatter[...] = jnp.where(slot_of(big_row) == big_slot, 1.0, 0.0).astype(BF16)
    big_row = iota((HALVES * group_rows, slots), 0)
    big_slot = iota((HALVES * group_rows, slots), 1)
    gather[...] = jnp.where(slot_of(big_row) == big_slot, 1.0, 0.0).astype(BF16)

    for g in range(GROUPS):
        first, hit = chosen(g)
        weight = jnp.where(first, weights[0:1, :], weights[1:2, :]) * hit
        for h in range(HALVES):
            mine = jnp.where(which_half == h, weight, 0.0).T
            high = mine.astype(BF16)
            comb[g, h] = high
            comb[g, HALVES + h] = (mine - high.astype(F32)).astype(BF16)

    for n in range(SENDS):
        arrived(n)
        pl.semaphore_signal(
            credit,
            inc=1,
            device_id={"ep": n_ep - 1 - e_pos, "tp": t_pos},
            device_id_type=MESH,
        )
        pl.semaphore_wait(credit, 1)
        if n + 1 < SENDS:
            dispatch(*order[n + AHEAD])
        else:
            for m in range(n + AHEAD, len(order)):
                dispatch(*order[m])
        if n == 0:

            @pl.when(e_pos % 2 == 0)
            def _():
                for j in range(2):
                    kv_copy(j).start()

        if n == 2:
            shared_send(1)

    size = qn.shape[1] // heads
    contract = (((1,), (1,)), ((), ()))
    diagonal = iota((rows, rows), 0) == iota((rows, rows), 1)

    def column(row):
        return jnp.sum(jnp.where(diagonal, row, 0.0), axis=1, keepdims=True)

    def as_row(col):
        return jnp.sum(jnp.where(diagonal, col, 0.0), axis=0, keepdims=True)

    def span_of(h):
        return slice(h * size, (h + 1) * size)

    def attend_pair(h, q, query_start, key_start, allowed):
        query_span = pl.ds(pl.multiple_of(query_start, rows), rows)
        key_span = pl.ds(pl.multiple_of(key_start, 2 * rows), 2 * rows)
        scores = jnp.concatenate(
            [
                lax.dot_general(
                    q, kv_buf[b, 0, :, span_of(h)], contract, preferred_element_type=F32
                )
                for b in range(2)
            ],
            axis=1,
        )
        scores = (
            scores * (size**-0.5)
            + column(cum[h : h + 1, query_span])
            - cum[h : h + 1, key_span]
        )
        if allowed is not None:
            scores = jnp.where(allowed, scores, -1e30)
        top = jnp.max(scores, axis=1, keepdims=True)
        probs = jnp.exp(scores - top)
        if allowed is not None:
            probs = jnp.where(allowed, probs, 0.0)
        norm = jnp.sum(probs, axis=1, keepdims=True)
        probs = probs.astype(BF16)
        mixed = jnp.dot(
            probs[:, :rows], kv_buf[0, 1, :, span_of(h)], preferred_element_type=F32
        ) + jnp.dot(probs[:, rows:], kv_buf[1, 1, :, span_of(h)], preferred_element_type=F32)
        return top, norm, mixed

    def compute(g):
        for c in range(SENDS):
            ordered = jnp.dot(gather[...], x_buf[g, c], preferred_element_type=F32).astype(BF16)
            for h in range(HALVES):
                start = h * half + c * x_wide
                x_rows[:, start : start + x_wide] = ordered[
                    h * group_rows : (h + 1) * group_rows
                ]

        def one(e, carry):
            copies = weight_copies(g, e)
            span = pl.ds(pl.multiple_of(e * expert_rows, expert_rows), expert_rows)
            copies[0].wait()
            copies[1].wait()
            both = jnp.dot(x_rows[span], wide_w[e], preferred_element_type=F32)
            gate = both[:, :hidden_width]
            hidden = (gate / (1.0 + jnp.exp(-gate)) * both[:, hidden_width:]).astype(BF16)
            copies[2].wait()
            for h in range(HALVES):
                at = pl.ds(pl.multiple_of(h * group_rows + e * expert_rows, expert_rows), expert_rows)
                for c in range(2):
                    cols = slice(c * half // 2, (c + 1) * half // 2)
                    y_rows[at, cols] = jnp.dot(
                        hidden,
                        down_w[e, :, h * half + c * half // 2 : h * half + (c + 1) * half // 2],
                        preferred_element_type=F32,
                    ).astype(BF16)
            if g + 1 < GROUPS:
                for copy in weight_copies(g + 1, e):
                    copy.start()
            return carry

        lax.fori_loop(0, per, one, 0)

    def place(g, c):
        y_buf[g, c] = jnp.dot(
            scatter[...], y_rows[:, c * y_wide : (c + 1) * y_wide], preferred_element_type=F32
        ).astype(BF16)

    def give(g, c):
        pltpu.make_async_copy(
            y_buf.at[g, c, rows_of(me)], r_buf.at[g, c, rows_of(me)], y_own.at[g, c]
        ).start()
        to_peers(y_buf.at[g, c], r_buf.at[g, c], y_send.at[g], y_recv.at[g, c])

    def give_back(g):
        place(g, 0)
        for c in range(1, RETURNS):
            place(g, c)
            give(g, c - 1)

    compute(0)
    shared_send(2)
    for c in range(RETURNS):
        place(0, c)
    sent(GROUPS - 1, SENDS - 2)
    give(0, 0)
    sent(GROUPS - 1, SENDS - 1)

    @pl.when(e_pos >= 2)
    def _():
        q_copy().start()

    for c in range(1, RETURNS):
        give(0, c)

    @pl.when(e_pos % 2 == 1)
    def _():
        for j in range(2):
            kv_copy(j).wait_recv()

    at = (e_pos % 2) * rows + iota((rows, 2 * rows), 0)
    allowed = iota((rows, 2 * rows), 1) <= at
    near = [
        attend_pair(h, qn[:, span_of(h)], e_pos * rows, (e_pos // 2) * 2 * rows, allowed)
        for h in range(heads)
    ]
    for h in range(heads):
        near_sum[:, span_of(h)] = near[h][2]

    shared_send(3)
    for n in range(SENDS, len(order)):
        arrived(n)
    compute(1)
    give_back(1)

    @pl.when(e_pos < 2)
    def _():
        far_in[...] = jnp.zeros(far_in.shape, BF16)
        stat_in[0:heads] = jnp.full((heads, rows), -1e30, F32)
        stat_in[heads:] = jnp.zeros((stat_in.shape[0] - heads, rows), F32)

    give(1, RETURNS - 1)

    @pl.when(e_pos == 1)
    def _():
        for i in range(2):
            pltpu.make_async_copy(q_far.at[i], q_far.at[i], q_recv.at[i]).wait()
            for h in range(heads):
                top, norm, mixed = attend_pair(
                    h, q_far[i, :, span_of(h)], (2 + i) * rows, 0, None
                )
                far_out[i, :, span_of(h)] = mixed.astype(BF16)
                stat_out[i, h : h + 1] = as_row(top)
                stat_out[i, heads + h : heads + h + 1] = as_row(norm)

    def far_copies(i):
        return (
            pltpu.make_async_remote_copy(
                src_ref=far_out.at[i],
                dst_ref=far_in,
                send_sem=far_send.at[i, 0],
                recv_sem=far_recv.at[0],
                device_id={"ep": 2 + i},
                device_id_type=MESH,
            ),
            pltpu.make_async_remote_copy(
                src_ref=stat_out.at[i],
                dst_ref=stat_in,
                send_sem=far_send.at[i, 1],
                recv_sem=far_recv.at[1],
                device_id={"ep": 2 + i},
                device_id_type=MESH,
            ),
        )

    across_copies = []
    for c in range(SHARED):
        cols = pl.ds(c * sh_wide, sh_wide)
        pltpu.make_async_copy(
            sh_buf.at[across, :, cols], sh_buf.at[across, :, cols], sh_recv.at[1, c]
        ).wait()
        copy = pltpu.make_async_remote_copy(
            src_ref=sh_buf.at[across, :, cols],
            dst_ref=sh_buf.at[across, :, cols],
            send_sem=sf_send.at[c],
            recv_sem=sf_recv.at[c],
            device_id={"tp": mate},
            device_id_type=MESH,
        )
        copy.start()
        across_copies.append(copy)
    @pl.when(e_pos == 1)
    def _():
        for i in range(2):
            for copy in far_copies(i):
                copy.start()

    for copy in own_shared:
        copy.wait()
    third = mate + 2 - 4 * (mate // 2)
    for c in range(SHARED):
        cols = pl.ds(c * sh_wide, sh_wide)
        pltpu.make_async_copy(
            sh_buf.at[mate, :, cols], sh_buf.at[mate, :, cols], sh_recv.at[0, c]
        ).wait()
        pltpu.make_async_copy(
            sh_buf.at[third, :, cols], sh_buf.at[third, :, cols], sf_recv.at[c]
        ).wait()
    hidden_parts = []
    for blk in range(n_tp):
        both = [
            sum(
                lax.dot_general(
                    normed[h * rows : (h + 1) * rows, :],
                    sh_buf[blk, j * part : (j + 1) * part, h * half : (h + 1) * half],
                    contract,
                    preferred_element_type=F32,
                )
                for h in range(HALVES)
            )
            for j in range(2)
        ]
        hidden_parts.append((both[0] / (1.0 + jnp.exp(-both[0])) * both[1]).astype(BF16))
    narrow = dim // 8
    for c in range(8):
        cols = slice(c * narrow, (c + 1) * narrow)
        summed = jnp.zeros((rows, narrow), F32)
        for blk in range(n_tp):
            piece = jnp.dot(
                hidden_parts[blk],
                sh_buf[blk, 2 * part : 3 * part, cols],
                preferred_element_type=F32,
            )
            summed += piece.astype(BF16).astype(F32)
        total[:, cols] = summed.astype(BF16).astype(F32)

    def returned(g, c):
        pltpu.make_async_copy(
            r_buf.at[g, c, pl.ds(0, peer_rows)],
            r_buf.at[g, c, pl.ds(0, peer_rows)],
            y_recv.at[g, c],
        ).wait()
        pltpu.make_async_copy(
            r_buf.at[g, c, pl.ds(0, block)], r_buf.at[g, c, pl.ds(0, block)], y_own.at[g, c]
        ).wait()
        back = r_buf[g, c]
        for h in range(HALVES):
            cols = slice(h * half + c * y_wide, h * half + (c + 1) * y_wide)
            routed = jnp.dot(comb[g, h], back, preferred_element_type=F32) + jnp.dot(
                comb[g, HALVES + h], back, preferred_element_type=F32
            )
            if g + 1 < GROUPS:
                total[:, cols] += routed
            else:
                res_ref[:, cols] = (total[:, cols] + routed).astype(BF16)

    for g in range(GROUPS - 1):
        for c in range(RETURNS):
            returned(g, c)

    @pl.when(e_pos >= 2)
    def _():
        for copy in far_copies(0):
            copy.wait_recv()

    parts = []
    for h in range(heads):
        top, norm, _ = near[h]
        far_top = column(stat_in[h : h + 1])
        best = jnp.maximum(top, far_top)
        near_scale = jnp.exp(top - best)
        far_scale = jnp.exp(far_top - best)
        far_norm = column(stat_in[heads + h : heads + h + 1])
        mixed = near_sum[:, span_of(h)] * near_scale + far_in[:, span_of(h)].astype(F32) * far_scale
        parts.append(mixed / (norm * near_scale + far_norm * far_scale))
    att_ref[...] = jnp.stack(parts, axis=1).astype(BF16)

    for c in range(RETURNS):
        returned(GROUPS - 1, c)

    for g, c in order[: len(order) - 2]:
        sent(g, c)
    for g in range(GROUPS):
        pltpu.make_async_copy(
            y_buf.at[g, :, pl.ds(0, peer_rows)],
            y_buf.at[g, :, pl.ds(0, peer_rows)],
            y_send.at[g],
        ).wait()
    for c in range(SHARED):
        cols = pl.ds(c * sh_wide, sh_wide)
        for s in range(2):
            pltpu.make_async_copy(
                sh_buf.at[t_pos, :, cols], sh_buf.at[t_pos, :, cols], sh_send.at[s, c]
            ).wait()
        across_copies[c].wait_send()

    @pl.when(e_pos % 2 == 0)
    def _():
        for j in range(2):
            kv_copy(j).wait_send()

    @pl.when(e_pos >= 2)
    def _():
        q_copy().wait_send()

    @pl.when(e_pos == 1)
    def _():
        for i in range(2):
            for copy in far_copies(i):
                copy.wait_send()


def fused_local(n_ep, n_tp, *args):
    (
        queries,
        key_vectors,
        values,
        forget_cum,
        query_gain,
        key_gain,
        tokens,
        norm_gain,
        routes,
        route_weights,
        expert_gate,
        expert_up,
        expert_down,
        shared_gate,
        shared_up,
        shared_down,
    ) = args
    rows, heads, size = queries.shape
    row_count, dim = tokens.shape
    local_count, _, hidden = expert_gate.shape
    count = n_ep * n_tp
    per = local_count // GROUPS
    slots = count * HALVES * per * CAP
    group_rows = count * per * CAP
    half = dim // HALVES
    part = shared_gate.shape[1]
    flat = heads * size
    hbm = pl.BlockSpec(memory_space=pltpu.HBM)
    sds = jax.ShapeDtypeStruct
    vmem = pltpu.VMEM
    dma = pltpu.SemaphoreType.DMA
    attended, routed = pl.pallas_call(
        functools.partial(fused_kernel, n_ep, n_tp, heads),
        out_shape=(vmem((rows, heads, size), BF16), vmem((row_count, dim), BF16)),
        in_specs=[hbm] * 16,
        out_specs=[pl.BlockSpec(memory_space=pltpu.VMEM)] * 2,
        scratch_shapes=[
            vmem((row_count, dim), BF16),
            vmem((1, dim), F32),
            vmem((TOP_K, row_count), jnp.int32),
            vmem((TOP_K, row_count), F32),
            vmem((rows, heads, size), BF16),
            vmem((rows, heads, size), BF16),
            vmem((rows, heads, size), BF16),
            vmem((1, size), F32),
            vmem((1, size), F32),
            vmem((heads, n_ep * rows), F32),
            vmem((HALVES * row_count, half), BF16),
            vmem((GROUPS, slots, HALVES * row_count), BF16),
            vmem((GROUPS, 2 * HALVES, row_count, slots), BF16),
            vmem((HALVES * group_rows, slots), BF16),
            vmem((slots, HALVES * group_rows), BF16),
            vmem((GROUPS, SENDS, slots, half // SENDS), BF16),
            vmem((GROUPS, SENDS, slots, half // SENDS), BF16),
            vmem((group_rows, dim), BF16),
            vmem((per, dim, 2 * hidden), BF16),
            vmem((per, hidden, dim), BF16),
            vmem((HALVES * group_rows, half), BF16),
            vmem((GROUPS, RETURNS, slots, half // RETURNS), BF16),
            vmem((GROUPS, RETURNS, slots, half // RETURNS), BF16),
            vmem((n_tp, 3 * part, dim), BF16),
            vmem((row_count, dim), F32),
            vmem((rows, flat), BF16),
            vmem((2, 2, rows, flat), BF16),
            vmem((2, rows, flat), BF16),
            vmem((2, rows, flat), BF16),
            vmem((rows, flat), BF16),
            vmem((2, 2 * heads, rows), F32),
            vmem((2 * heads, rows), F32),
            vmem((rows, flat), F32),
            dma((10,)),
            dma((per, 3)),
            dma((GROUPS, SENDS)),
            dma((GROUPS, SENDS)),
            dma((GROUPS, SENDS)),
            dma((GROUPS,)),
            dma((GROUPS, RETURNS)),
            dma((GROUPS, RETURNS)),
            dma((2, SHARED)),
            dma((2, SHARED)),
            dma((3,)),
            dma((SHARED,)),
            dma((SHARED,)),
            dma((2,)),
            dma((2,)),
            dma,
            dma((2,)),
            dma((2, 2)),
            dma((2,)),
            pltpu.SemaphoreType.REGULAR,
        ],
        compiler_params=pltpu.CompilerParams(
            collective_id=0, has_side_effects=True, vmem_limit_bytes=60 * 1024 * 1024
        ),
        name="fused",
    )(
        tokens,
        norm_gain.reshape(1, dim),
        routes.T,
        route_weights.T,
        queries,
        key_vectors,
        values,
        query_gain.reshape(1, size),
        key_gain.reshape(1, size),
        forget_cum.T,
        expert_gate,
        expert_up,
        expert_down,
        shared_gate.T,
        shared_up.T,
        shared_down,
    )
    return attended, routed


def local_of(mesh):
    n_ep, n_tp = mesh.shape["ep"], mesh.shape["tp"]

    def run(*args):
        experts = args[10]
        block = CAP * experts.shape[0]
        if n_tp == 4 and n_ep == 4 and block % 16 == 0 and args[15].shape[0] % 16 == 0:
            return fused_local(n_ep, n_tp, *args)
        return local(*args)

    return run


def solution(mesh):
    placed = (
        P(("grp", "ep"), "tp", None),
        P(("grp", "ep"), "tp", None),
        P(("grp", "ep"), "tp", None),
        P("grp", "tp"),
        P(),
        P(),
        P(("grp", "ep", "tp"), None),
        P(),
        P(("grp", "ep", "tp"), None),
        P(("grp", "ep", "tp"), None),
        P(("ep", "tp"), None, None),
        P(("ep", "tp"), None, None),
        P(("ep", "tp"), None, None),
        P(None, "tp"),
        P(None, "tp"),
        P("tp", None),
    )
    return jax.shard_map(
        local_of(mesh),
        mesh=mesh,
        in_specs=placed,
        out_specs=(P(("grp", "ep"), "tp", None), P(("grp", "ep", "tp"), None)),
        check_vma=False,
    )
```

```python
import functools
import jax
import jax.numpy as jnp
from jax import lax
from jax.experimental import pallas as pl
from jax.experimental.pallas import tpu as pltpu
from jax.sharding import PartitionSpec as P

MESH = pl.DeviceIdType.MESH
F32 = jnp.float32
BF16 = jnp.bfloat16
CAP = 2
GROUPS = 2
HALVES = 2
SENDS = 4
RETURNS = 4
SHARED = 4
AHEAD = 3

D = 4096
EXPERTS = 128
TOP_K = 2


def rms_rows(row_values, gain_vector):
    widened = row_values.astype(jnp.float32)
    inverse = lax.rsqrt(jnp.mean(widened * widened, axis=-1, keepdims=True) + 1e-06)
    return (widened * inverse * gain_vector).astype(jnp.bfloat16)


def attend(queries, key_vectors, values, forget_cum, query_gain, key_gain):
    query_norm = rms_rows(queries, query_gain)
    key_norm = rms_rows(key_vectors, key_gain)
    query_rows = query_norm.shape[0]
    head_count = query_norm.shape[1]
    head_size = query_norm.shape[2]
    first_query = lax.axis_index("ep") * query_rows
    query_positions = first_query + lax.iota(jnp.int32, query_rows)
    last_query = first_query + query_rows - 1
    query_cum = lax.dynamic_slice_in_dim(forget_cum, first_query, query_rows, 0).T
    scale_factor = head_size ** (-0.5)
    start_state = (
        jnp.full((head_count, query_rows), -1e30, jnp.float32),
        jnp.zeros((head_count, query_rows), jnp.float32),
        jnp.zeros((head_count, query_rows, head_size), jnp.float32),
    )
    key_part = lax.all_gather(key_norm, "ep", axis=0, tiled=True)
    value_part = lax.all_gather(values, "ep", axis=0, tiled=True)
    piece_rows = key_part.shape[0]

    def compute(inner_state):
        best_score, denominator, accumulated = inner_state
        cum_block = forget_cum.T
        scores = jnp.einsum(
            "qhd,khd->hqk", query_norm, key_part, preferred_element_type=jnp.float32
        )
        scores = scores * scale_factor + query_cum[:, :, None] - cum_block[:, None, :]
        key_positions = lax.iota(jnp.int32, piece_rows)
        allowed = (key_positions[None, :] <= query_positions[:, None])[None]
        scores = jnp.where(allowed, scores, -1e30)
        new_best = jnp.maximum(best_score, jnp.max(scores, axis=2))
        weights = jnp.where(allowed, jnp.exp(scores - new_best[:, :, None]), 0.0)
        denominator = jnp.sum(weights, axis=2)
        product = jnp.einsum(
            "hqk,khd->hqd",
            weights.astype(jnp.bfloat16),
            value_part,
            preferred_element_type=jnp.float32,
        )
        accumulated = product
        return (new_best, denominator, accumulated)

    best_score, denominator, accumulated = lax.cond(
        jnp.int32(0) <= last_query, compute, lambda inner_state: inner_state, start_state
    )
    return (accumulated / denominator[:, :, None]).transpose(1, 0, 2).astype(jnp.bfloat16)


def shared_expert(normed, shared_gate, shared_up, shared_down):
    row_count = normed.shape[0]
    whole_gate, whole_up, whole_down = (
        lax.all_gather(shared_gate, "tp", axis=1, tiled=True),
        lax.all_gather(shared_up, "tp", axis=1, tiled=True),
        lax.all_gather(shared_down, "tp", axis=0, tiled=True),
    )
    block_total = lax.axis_size("tp")
    gate_values = jnp.dot(normed, whole_gate, preferred_element_type=jnp.float32)
    upward = jnp.dot(normed, whole_up, preferred_element_type=jnp.float32)
    hidden_whole = (jax.nn.silu(gate_values) * upward).astype(jnp.bfloat16)
    part_width = whole_down.shape[0] // block_total
    hidden_blocks = hidden_whole.reshape(row_count, block_total, part_width)
    down_blocks = whole_down.reshape(block_total, part_width, whole_down.shape[1])
    partials = jnp.einsum(
        "rnp,npd->nrd", hidden_blocks, down_blocks, preferred_element_type=jnp.float32
    ).astype(jnp.bfloat16)
    return jnp.sum(partials.astype(jnp.float32), axis=0).astype(jnp.bfloat16)


def mixture(
    tokens,
    norm_gain,
    routes,
    route_weights,
    expert_gate,
    expert_up,
    expert_down,
    shared_gate,
    shared_up,
    shared_down,
):
    normed = rms_rows(tokens, norm_gain)
    row_count = tokens.shape[0]
    shared_out = shared_expert(normed, shared_gate, shared_up, shared_down)
    flat_routes = routes.reshape(-1)
    choice_count = flat_routes.shape[0]
    one_hot = (flat_routes[:, None] == lax.iota(jnp.int32, EXPERTS)[None, :]).astype(jnp.int32)
    slot_rank = jnp.sum((jnp.cumsum(one_hot, axis=0) - one_hot) * one_hot, axis=1)
    slot_index = slot_rank * EXPERTS + flat_routes
    slot_ids = lax.iota(jnp.int32, CAP * EXPERTS)
    matches = slot_index[None, :] == slot_ids[:, None]
    source_row = jnp.sum(
        jnp.where(matches, lax.iota(jnp.int32, choice_count)[None, :] // TOP_K, 0), axis=1
    )
    filled = jnp.any(matches, axis=1)
    outgoing = jnp.where(filled[:, None], normed[source_row], jnp.zeros((), jnp.bfloat16)).reshape(
        CAP, EXPERTS, D
    )
    arrived = lax.all_to_all(outgoing, ("ep", "tp"), split_axis=1, concat_axis=1, tiled=True)
    local_count = expert_gate.shape[0]
    grouped = arrived.reshape(CAP, -1, local_count, D)
    gate_values = jnp.einsum(
        "csed,edf->csef", grouped, expert_gate, preferred_element_type=jnp.float32
    )
    upward = jnp.einsum("csed,edf->csef", grouped, expert_up, preferred_element_type=jnp.float32)
    hidden = (jax.nn.silu(gate_values) * upward).astype(jnp.bfloat16)
    produced = (
        jnp.einsum("csef,efd->csed", hidden, expert_down, preferred_element_type=jnp.float32)
        .astype(jnp.bfloat16)
        .reshape(CAP, -1, D)
    )
    returned = lax.all_to_all(produced, ("ep", "tp"), split_axis=1, concat_axis=1, tiled=True)
    picked_rows = returned.reshape(CAP * EXPERTS, D)[slot_index].reshape(row_count, TOP_K, D)
    routed = jnp.sum(route_weights[:, :, None] * picked_rows.astype(jnp.float32), axis=1)
    return (shared_out.astype(jnp.float32) + routed).astype(jnp.bfloat16)


def local(
    queries,
    key_vectors,
    values,
    forget_cum,
    query_gain,
    key_gain,
    tokens,
    norm_gain,
    routes,
    route_weights,
    expert_gate,
    expert_up,
    expert_down,
    shared_gate,
    shared_up,
    shared_down,
):
    attended = attend(queries, key_vectors, values, forget_cum, query_gain, key_gain)
    routed_output = mixture(
        tokens,
        norm_gain,
        routes,
        route_weights,
        expert_gate,
        expert_up,
        expert_down,
        shared_gate,
        shared_up,
        shared_down,
    )
    return (attended, routed_output)


def rms_heads(wide, gain, heads):
    pieces = []
    for h in range(heads):
        part = wide[:, h, :]
        inverse = lax.rsqrt(jnp.mean(part * part, axis=-1, keepdims=True) + 1e-06)
        pieces.append((part * inverse * gain).astype(BF16))
    return jnp.concatenate(pieces, axis=1)


def iota(shape, axis):
    return lax.broadcasted_iota(jnp.int32, shape, axis)


def fused_kernel(
    n_ep,
    n_tp,
    heads,
    tokens_ref,
    gain_ref,
    routes_ref,
    weights_ref,
    q_ref,
    k_ref,
    v_ref,
    qg_ref,
    kg_ref,
    cum_ref,
    gate_ref,
    up_ref,
    down_ref,
    sg_ref,
    su_ref,
    sd_ref,
    att_ref,
    res_ref,
    tok,
    gain,
    routes,
    weights,
    q_in,
    k_in,
    v_in,
    q_gain,
    k_gain,
    cum,
    normed,
    pick,
    comb,
    gather,
    scatter,
    outgoing,
    x_buf,
    x_rows,
    wide_w,
    down_w,
    y_rows,
    y_buf,
    r_buf,
    sh_buf,
    total,
    qn,
    kv_buf,
    q_far,
    far_out,
    far_in,
    stat_out,
    stat_in,
    near_sum,
    in_sem,
    w_sem,
    x_send,
    x_recv,
    y_send,
    y_recv,
    sh_send,
    sh_recv,
    sh_own,
    sf_send,
    sf_recv,
    kv_send,
    kv_recv,
    q_send,
    q_recv,
    far_send,
    far_recv,
    credit,
):
    e_pos = lax.axis_index("ep")
    t_pos = lax.axis_index("tp")
    count = n_ep * n_tp
    me = e_pos * n_tp + t_pos
    local_count = gate_ref.shape[0]
    per = local_count // GROUPS
    hidden_width = gate_ref.shape[2]
    block = HALVES * per * CAP
    slots = count * block
    expert_rows = count * CAP
    group_rows = per * expert_rows
    rows, dim = tok.shape
    half = dim // HALVES
    x_wide = half // SENDS
    y_wide = half // RETURNS
    peer_rows = (count - 1) * block

    def device(i):
        return {"ep": i // n_tp, "tp": i % n_tp}

    barrier = pltpu.get_barrier_semaphore()

    def greet(i, carry):
        pl.semaphore_signal(
            barrier, inc=1, device_id=device((me + i) % count), device_id_type=MESH
        )
        return carry

    lax.fori_loop(1, count, greet, 0)
    inputs = [
        pltpu.make_async_copy(src, dst, in_sem.at[i])
        for i, (src, dst) in enumerate(
            (
                (routes_ref, routes),
                (tokens_ref, tok),
                (gain_ref, gain),
                (weights_ref, weights),
                (k_ref, k_in),
                (v_ref, v_in),
                (q_ref, q_in),
                (qg_ref, q_gain),
                (kg_ref, k_gain),
                (cum_ref, cum),
            )
        )
    ]
    for copy in inputs:
        copy.start()

    def weight_copies(g, e):
        n = g * per + e
        return (
            pltpu.make_async_copy(
                gate_ref.at[n], wide_w.at[e, :, pl.ds(0, hidden_width)], w_sem.at[e, 0]
            ),
            pltpu.make_async_copy(
                up_ref.at[n], wide_w.at[e, :, pl.ds(hidden_width, hidden_width)], w_sem.at[e, 1]
            ),
            pltpu.make_async_copy(down_ref.at[n], down_w.at[e], w_sem.at[e, 2]),
        )

    def first_weights(e, carry):
        for copy in weight_copies(0, e):
            copy.start()
        return carry

    shared_refs = (sg_ref, su_ref, sd_ref)
    part = sd_ref.shape[0]
    own_shared = [
        pltpu.make_async_copy(src, sh_buf.at[t_pos, pl.ds(j * part, part)], sh_own)
        for j, src in enumerate(shared_refs)
    ]

    inputs[0].wait()
    inputs[3].wait()
    lax.fori_loop(0, per, first_weights, 0)
    for copy in own_shared:
        copy.start()

    r = iota((slots, rows), 0)
    which_half = (r % block) // (per * CAP)
    before = jnp.where(iota((rows, rows), 0) < iota((rows, rows), 1), 1.0, 0.0).astype(BF16)

    def chosen(g):
        expert = (r // block) * local_count + g * per + (r % (per * CAP)) // CAP
        first = expert == routes[0:1, :]
        named = jnp.where(first | (expert == routes[1:2, :]), 1.0, 0.0)
        earlier = jnp.dot(named.astype(BF16), before, preferred_element_type=F32)
        return first, jnp.where(earlier == (r % CAP).astype(F32), named, 0.0)

    def fill_pick(g):
        _, hit = chosen(g)
        for h in range(HALVES):
            pick[g, :, h * rows : (h + 1) * rows] = jnp.where(which_half == h, hit, 0.0).astype(
                BF16
            )

    fill_pick(0)
    inputs[1].wait()
    inputs[2].wait()
    wide = tok[...].astype(F32)
    inverse = lax.rsqrt(jnp.mean(wide * wide, axis=-1, keepdims=True) + 1e-06)
    step = half // 4
    for h in range(HALVES):
        for c in range(4):
            cols = slice(h * half + c * step, h * half + (c + 1) * step)
            normed[h * rows : (h + 1) * rows, c * step : (c + 1) * step] = (
                tok[:, cols].astype(F32) * inverse * gain[:, cols]
            ).astype(BF16)
    pl.semaphore_wait(barrier, count - 1)

    def rows_of(i):
        return pl.ds(pl.multiple_of(i * block, block), block)

    beside = e_pos + 1 - 2 * (e_pos % 2)
    opposite = 1 - e_pos // 2
    inner = opposite + 1
    outer = opposite * (n_ep - 1)
    every = ((e_pos + 2) % n_ep, n_ep - 1 - e_pos, beside, e_pos)

    def to_peers(src, dst, send_sem, recv_sem, planes):
        for e in planes:

            def send(j, carry):
                peer = e * n_tp + (t_pos + j) % n_tp
                pltpu.make_async_remote_copy(
                    src_ref=src.at[rows_of(peer)],
                    dst_ref=dst.at[rows_of(me)],
                    send_sem=send_sem,
                    recv_sem=recv_sem,
                    device_id=device(peer),
                    device_id_type=MESH,
                ).start()
                return carry

            lax.fori_loop(1 if e is e_pos else 0, n_tp, send, 0)

    def pick_rows(g, c):
        outgoing[g, c] = jnp.dot(
            pick[g], normed[:, c * x_wide : (c + 1) * x_wide], preferred_element_type=F32
        ).astype(BF16)
        x_buf[g, c, rows_of(me)] = outgoing[g, c, rows_of(me)]

    def dispatch(g, c):
        to_peers(outgoing.at[g, c], x_buf.at[g, c], x_send.at[g], x_recv.at[g, c], every)

    mate = t_pos + 1 - 2 * (t_pos % 2)
    across = (t_pos + 2) % n_tp
    sh_wide = dim // SHARED

    def shared_send(c):
        cols = pl.ds(c * sh_wide, sh_wide)
        for s, target in enumerate((mate, across)):
            for j, src in enumerate(shared_refs):
                pltpu.make_async_remote_copy(
                    src_ref=src.at[:, cols],
                    dst_ref=sh_buf.at[t_pos, pl.ds(j * part, part), cols],
                    send_sem=sh_send,
                    recv_sem=sh_recv.at[s],
                    device_id={"tp": target},
                    device_id_type=MESH,
                ).start()

    order = [(g, c) for g in range(GROUPS) for c in range(SENDS)]

    def arrived(n):
        g, c = order[n]
        away = x_buf.at[g, c, pl.ds(0, peer_rows)]
        pltpu.make_async_copy(away, away, x_recv.at[g, c]).wait()

    def exchange_credit():
        pl.semaphore_signal(
            credit,
            inc=1,
            device_id={"ep": n_ep - 1 - e_pos, "tp": t_pos},
            device_id_type=MESH,
        )
        pl.semaphore_wait(credit, 1)

    pick_rows(*order[0])
    for n in range(1, AHEAD):
        pick_rows(*order[n])
        dispatch(*order[n - 1])
    for n in range(AHEAD, SENDS):
        pick_rows(*order[n])
    dispatch(*order[AHEAD - 1])
    for g in range(1, GROUPS):
        fill_pick(g)
    shared_send(0)

    for copy in inputs[4:]:
        copy.wait()
    qn[...] = rms_heads(q_in[...].astype(F32), q_gain[...], heads)
    kv_buf[e_pos % 2, 0] = rms_heads(k_in[...].astype(F32), k_gain[...], heads)
    held = v_in[...].astype(F32)
    kv_buf[e_pos % 2, 1] = jnp.concatenate(
        [held[:, h, :].astype(BF16) for h in range(heads)], axis=1
    )

    @pl.when(e_pos % 2 == 0)
    def _():
        kv_buf[1] = jnp.zeros(kv_buf.shape[1:], BF16)

    for g in range(1, GROUPS):
        for c in range(SENDS):
            pick_rows(g, c)

    def kv_copy():
        return pltpu.make_async_remote_copy(
            src_ref=kv_buf.at[0],
            dst_ref=kv_buf.at[0],
            send_sem=kv_send,
            recv_sem=kv_recv,
            device_id={"ep": jnp.minimum(e_pos + 1, n_ep - 1)},
            device_id_type=MESH,
        )

    far_index = jnp.maximum(e_pos - 2, 0)

    def q_copy():
        return pltpu.make_async_remote_copy(
            src_ref=qn,
            dst_ref=q_far.at[far_index],
            send_sem=q_send,
            recv_sem=q_recv.at[far_index],
            device_id={"ep": 1},
            device_id_type=MESH,
        )

    big_row = iota((slots, HALVES * group_rows), 1)
    big_slot = iota((slots, HALVES * group_rows), 0)

    def slot_of(n):
        h = n // group_rows
        e = (n % group_rows) // expert_rows
        src = (n % expert_rows) // CAP
        return src * block + h * (per * CAP) + e * CAP + n % CAP

    scatter[...] = jnp.where(slot_of(big_row) == big_slot, 1.0, 0.0).astype(BF16)
    big_row = iota((HALVES * group_rows, slots), 0)
    big_slot = iota((HALVES * group_rows, slots), 1)
    gather[...] = jnp.where(slot_of(big_row) == big_slot, 1.0, 0.0).astype(BF16)

    for g in range(GROUPS):
        first, hit = chosen(g)
        weight = jnp.where(first, weights[0:1, :], weights[1:2, :]) * hit
        for h in range(HALVES):
            mine = jnp.where(which_half == h, weight, 0.0).T
            high = mine.astype(BF16)
            comb[g, h] = high
            comb[g, HALVES + h] = (mine - high.astype(F32)).astype(BF16)

    for n in range(SENDS):
        arrived(n)
        exchange_credit()
        if n + 1 < SENDS:
            dispatch(*order[n + AHEAD])
        else:
            for m in range(n + AHEAD, len(order)):
                dispatch(*order[m])
        if n == 0:

            @pl.when(e_pos % 2 == 0)
            def _():
                kv_copy().start()

            @pl.when(e_pos >= 2)
            def _():
                q_copy().start()

        if n == 2:
            shared_send(1)

    size = qn.shape[1] // heads
    contract = (((1,), (1,)), ((), ()))
    diagonal = iota((rows, rows), 0) == iota((rows, rows), 1)

    def column(row):
        return jnp.sum(jnp.where(diagonal, row, 0.0), axis=1, keepdims=True)

    def as_row(col):
        return jnp.sum(jnp.where(diagonal, col, 0.0), axis=0, keepdims=True)

    def span_of(h):
        return slice(h * size, (h + 1) * size)

    def attend_pair(h, q, query_start, key_start, allowed):
        query_span = pl.ds(pl.multiple_of(query_start, rows), rows)
        key_span = pl.ds(pl.multiple_of(key_start, 2 * rows), 2 * rows)
        scores = jnp.concatenate(
            [
                lax.dot_general(
                    q, kv_buf[b, 0, :, span_of(h)], contract, preferred_element_type=F32
                )
                for b in range(2)
            ],
            axis=1,
        )
        scores = (
            scores * (size**-0.5)
            + column(cum[h : h + 1, query_span])
            - cum[h : h + 1, key_span]
        )
        if allowed is not None:
            scores = jnp.where(allowed, scores, -1e30)
        top = jnp.max(scores, axis=1, keepdims=True)
        probs = jnp.exp(scores - top)
        if allowed is not None:
            probs = jnp.where(allowed, probs, 0.0)
        norm = jnp.sum(probs, axis=1, keepdims=True)
        probs = probs.astype(BF16)
        mixed = jnp.dot(
            probs[:, :rows], kv_buf[0, 1, :, span_of(h)], preferred_element_type=F32
        ) + jnp.dot(probs[:, rows:], kv_buf[1, 1, :, span_of(h)], preferred_element_type=F32)
        return top, norm, mixed

    def compute(g):
        for c in range(SENDS):
            ordered = jnp.dot(gather[...], x_buf[g, c], preferred_element_type=F32).astype(BF16)
            for h in range(HALVES):
                start = h * half + c * x_wide
                x_rows[:, start : start + x_wide] = ordered[
                    h * group_rows : (h + 1) * group_rows
                ]

        def one(e, carry):
            copies = weight_copies(g, e)
            span = pl.ds(pl.multiple_of(e * expert_rows, expert_rows), expert_rows)
            copies[0].wait()
            copies[1].wait()
            both = jnp.dot(x_rows[span], wide_w[e], preferred_element_type=F32)
            gate = both[:, :hidden_width]
            hidden = (gate / (1.0 + jnp.exp(-gate)) * both[:, hidden_width:]).astype(BF16)
            copies[2].wait()
            for h in range(HALVES):
                at = pl.ds(pl.multiple_of(h * group_rows + e * expert_rows, expert_rows), expert_rows)
                for c in range(2):
                    cols = slice(c * half // 2, (c + 1) * half // 2)
                    y_rows[at, cols] = jnp.dot(
                        hidden,
                        down_w[e, :, h * half + c * half // 2 : h * half + (c + 1) * half // 2],
                        preferred_element_type=F32,
                    ).astype(BF16)
            if g + 1 < GROUPS:
                for copy in weight_copies(g + 1, e):
                    copy.start()
            return carry

        lax.fori_loop(0, per, one, 0)

    def place(g, c):
        y_buf[g, c] = jnp.dot(
            scatter[...], y_rows[:, c * y_wide : (c + 1) * y_wide], preferred_element_type=F32
        ).astype(BF16)
        r_buf[g, c, rows_of(me)] = y_buf[g, c, rows_of(me)]

    def give(g, c, planes):
        arrival = c if g + 1 == GROUPS else RETURNS
        to_peers(y_buf.at[g, c], r_buf.at[g, c], y_send.at[g], y_recv.at[arrival], planes)

    compute(0)
    shared_send(2)
    for c in range(RETURNS):
        place(0, c)
    @pl.when(e_pos % 2 == 1)
    def _():
        kv_copy().wait_recv()

    at = (e_pos % 2) * rows + iota((rows, 2 * rows), 0)
    allowed = iota((rows, 2 * rows), 1) <= at
    near = [
        attend_pair(h, qn[:, span_of(h)], e_pos * rows, (e_pos // 2) * 2 * rows, allowed)
        for h in range(heads)
    ]
    for h in range(heads):
        near_sum[:, span_of(h)] = near[h][2]

    @pl.when(e_pos == 1)
    def _():
        for i in range(2):
            pltpu.make_async_copy(q_far.at[i], q_far.at[i], q_recv.at[i]).wait()
            for h in range(heads):
                top, norm, mixed = attend_pair(
                    h, q_far[i, :, span_of(h)], (2 + i) * rows, 0, None
                )
                far_out[i, :, span_of(h)] = mixed.astype(BF16)
                stat_out[i, h : h + 1] = as_row(top)
                stat_out[i, heads + h : heads + h + 1] = as_row(norm)

    def far_copies(i):
        return (
            pltpu.make_async_remote_copy(
                src_ref=far_out.at[i],
                dst_ref=far_in,
                send_sem=far_send.at[i, 0],
                recv_sem=far_recv.at[0],
                device_id={"ep": 2 + i},
                device_id_type=MESH,
            ),
            pltpu.make_async_remote_copy(
                src_ref=stat_out.at[i],
                dst_ref=stat_in,
                send_sem=far_send.at[i, 1],
                recv_sem=far_recv.at[1],
                device_id={"ep": 2 + i},
                device_id_type=MESH,
            ),
        )

    shared_send(3)
    for n in range(SENDS, len(order)):
        arrived(n)
        if n == SENDS:

            @pl.when(e_pos == 1)
            def _():
                for i in range(2):
                    for copy in far_copies(i):
                        copy.start()

        if n + 2 == len(order):
            exchange_credit()
            give(0, 0, every)
    exchange_credit()
    for c in range(1, RETURNS):
        give(0, c, every)
    compute(1)
    first_planes = (outer, beside, e_pos)
    place(1, 0)
    for c in range(1, RETURNS):
        place(1, c)
        give(1, c - 1, first_planes)

    @pl.when(e_pos < 2)
    def _():
        far_in[...] = jnp.zeros(far_in.shape, BF16)
        stat_in[0:heads] = jnp.full((heads, rows), -1e30, F32)
        stat_in[heads:] = jnp.zeros((stat_in.shape[0] - heads, rows), F32)

    give(1, RETURNS - 1, first_planes)
    for c in range(RETURNS):
        give(1, c, (inner,))

    def whole(i):
        return sh_buf.at[i]

    pltpu.make_async_copy(whole(across), whole(across), sh_recv.at[1]).wait()
    across_copy = pltpu.make_async_remote_copy(
        src_ref=whole(across),
        dst_ref=whole(across),
        send_sem=sf_send,
        recv_sem=sf_recv,
        device_id={"tp": mate},
        device_id_type=MESH,
    )
    across_copy.start()
    pltpu.make_async_copy(whole(t_pos), whole(t_pos), sh_own).wait()
    third = mate + 2 - 4 * (mate // 2)
    pltpu.make_async_copy(whole(mate), whole(mate), sh_recv.at[0]).wait()
    pltpu.make_async_copy(whole(third), whole(third), sf_recv).wait()
    hidden_parts = []
    for blk in range(n_tp):
        both = [
            sum(
                lax.dot_general(
                    normed[h * rows : (h + 1) * rows, :],
                    sh_buf[blk, j * part : (j + 1) * part, h * half : (h + 1) * half],
                    contract,
                    preferred_element_type=F32,
                )
                for h in range(HALVES)
            )
            for j in range(2)
        ]
        hidden_parts.append((both[0] / (1.0 + jnp.exp(-both[0])) * both[1]).astype(BF16))
    narrow = dim // 8
    for c in range(8):
        cols = slice(c * narrow, (c + 1) * narrow)
        summed = jnp.zeros((rows, narrow), F32)
        for blk in range(n_tp):
            piece = jnp.dot(
                hidden_parts[blk],
                sh_buf[blk, 2 * part : 3 * part, cols],
                preferred_element_type=F32,
            )
            summed += piece.astype(BF16).astype(F32)
        total[:, cols] = summed.astype(BF16).astype(F32)

    def returned(g, c):
        back = r_buf[g, c]
        for h in range(HALVES):
            cols = slice(h * half + c * y_wide, h * half + (c + 1) * y_wide)
            routed = jnp.dot(comb[g, h], back, preferred_element_type=F32) + jnp.dot(
                comb[g, HALVES + h], back, preferred_element_type=F32
            )
            if g + 1 < GROUPS:
                total[:, cols] += routed
            else:
                res_ref[:, cols] = (total[:, cols] + routed).astype(BF16)

    @pl.when(e_pos >= 2)
    def _():
        for copy in far_copies(0):
            copy.wait_recv()

    parts = []
    for h in range(heads):
        top, norm, _ = near[h]
        far_top = column(stat_in[h : h + 1])
        best = jnp.maximum(top, far_top)
        near_scale = jnp.exp(top - best)
        far_scale = jnp.exp(far_top - best)
        far_norm = column(stat_in[heads + h : heads + h + 1])
        mixed = near_sum[:, span_of(h)] * near_scale + far_in[:, span_of(h)].astype(F32) * far_scale
        parts.append(mixed / (norm * near_scale + far_norm * far_scale))
    att_ref[...] = jnp.stack(parts, axis=1).astype(BF16)

    away = r_buf.at[0, :, pl.ds(0, peer_rows)]
    pltpu.make_async_copy(away, away, y_recv.at[RETURNS]).wait()
    for c in range(RETURNS):
        returned(0, c)

    for c in range(RETURNS):
        away = r_buf.at[1, c, pl.ds(0, peer_rows)]
        pltpu.make_async_copy(away, away, y_recv.at[c]).wait()
        returned(1, c)

    for g in range(GROUPS):
        for buf, sem in ((x_buf, x_send), (y_buf, y_send)):
            away = buf.at[g, :, pl.ds(0, peer_rows)]
            pltpu.make_async_copy(away, away, sem.at[g]).wait()
    pair = sh_buf.at[pl.ds(0, 2)]
    pltpu.make_async_copy(pair, pair, sh_send).wait()
    across_copy.wait_send()

    @pl.when(e_pos % 2 == 0)
    def _():
        kv_copy().wait_send()

    @pl.when(e_pos >= 2)
    def _():
        q_copy().wait_send()

    @pl.when(e_pos == 1)
    def _():
        for i in range(2):
            for copy in far_copies(i):
                copy.wait_send()


def fused_local(n_ep, n_tp, *args):
    (
        queries,
        key_vectors,
        values,
        forget_cum,
        query_gain,
        key_gain,
        tokens,
        norm_gain,
        routes,
        route_weights,
        expert_gate,
        expert_up,
        expert_down,
        shared_gate,
        shared_up,
        shared_down,
    ) = args
    rows, heads, size = queries.shape
    row_count, dim = tokens.shape
    local_count, _, hidden = expert_gate.shape
    count = n_ep * n_tp
    per = local_count // GROUPS
    slots = count * HALVES * per * CAP
    group_rows = count * per * CAP
    half = dim // HALVES
    part = shared_gate.shape[1]
    flat = heads * size
    hbm = pl.BlockSpec(memory_space=pltpu.HBM)
    sds = jax.ShapeDtypeStruct
    vmem = pltpu.VMEM
    dma = pltpu.SemaphoreType.DMA
    attended, routed = pl.pallas_call(
        functools.partial(fused_kernel, n_ep, n_tp, heads),
        out_shape=(vmem((rows, heads, size), BF16), vmem((row_count, dim), BF16)),
        in_specs=[hbm] * 16,
        out_specs=[pl.BlockSpec(memory_space=pltpu.VMEM)] * 2,
        scratch_shapes=[
            vmem((row_count, dim), BF16),
            vmem((1, dim), F32),
            vmem((TOP_K, row_count), jnp.int32),
            vmem((TOP_K, row_count), F32),
            vmem((rows, heads, size), BF16),
            vmem((rows, heads, size), BF16),
            vmem((rows, heads, size), BF16),
            vmem((1, size), F32),
            vmem((1, size), F32),
            vmem((heads, n_ep * rows), F32),
            vmem((HALVES * row_count, half), BF16),
            vmem((GROUPS, slots, HALVES * row_count), BF16),
            vmem((GROUPS, 2 * HALVES, row_count, slots), BF16),
            vmem((HALVES * group_rows, slots), BF16),
            vmem((slots, HALVES * group_rows), BF16),
            vmem((GROUPS, SENDS, slots, half // SENDS), BF16),
            vmem((GROUPS, SENDS, slots, half // SENDS), BF16),
            vmem((group_rows, dim), BF16),
            vmem((per, dim, 2 * hidden), BF16),
            vmem((per, hidden, dim), BF16),
            vmem((HALVES * group_rows, half), BF16),
            vmem((GROUPS, RETURNS, slots, half // RETURNS), BF16),
            vmem((GROUPS, RETURNS, slots, half // RETURNS), BF16),
            vmem((n_tp, 3 * part, dim), BF16),
            vmem((row_count, dim), F32),
            vmem((rows, flat), BF16),
            vmem((2, 2, rows, flat), BF16),
            vmem((2, rows, flat), BF16),
            vmem((2, rows, flat), BF16),
            vmem((rows, flat), BF16),
            vmem((2, 2 * heads, rows), F32),
            vmem((2 * heads, rows), F32),
            vmem((rows, flat), F32),
            dma((10,)),
            dma((per, 3)),
            dma((GROUPS,)),
            dma((GROUPS, SENDS)),
            dma((GROUPS,)),
            dma((RETURNS + 1,)),
            dma,
            dma((2,)),
            dma,
            dma,
            dma,
            dma,
            dma,
            dma,
            dma((2,)),
            dma((2, 2)),
            dma((2,)),
            pltpu.SemaphoreType.REGULAR,
        ],
        compiler_params=pltpu.CompilerParams(
            collective_id=0, has_side_effects=True, vmem_limit_bytes=60 * 1024 * 1024
        ),
        name="fused",
    )(
        tokens,
        norm_gain.reshape(1, dim),
        routes.T,
        route_weights.T,
        queries,
        key_vectors,
        values,
        query_gain.reshape(1, size),
        key_gain.reshape(1, size),
        forget_cum.T,
        expert_gate,
        expert_up,
        expert_down,
        shared_gate.T,
        shared_up.T,
        shared_down,
    )
    return attended, routed


def local_of(mesh):
    n_ep, n_tp = mesh.shape["ep"], mesh.shape["tp"]

    def run(*args):
        experts = args[10]
        block = CAP * experts.shape[0]
        if n_tp == 4 and n_ep == 4 and block % 16 == 0 and args[15].shape[0] % 16 == 0:
            return fused_local(n_ep, n_tp, *args)
        return local(*args)

    return run


def solution(mesh):
    placed = (
        P(("grp", "ep"), "tp", None),
        P(("grp", "ep"), "tp", None),
        P(("grp", "ep"), "tp", None),
        P("grp", "tp"),
        P(),
        P(),
        P(("grp", "ep", "tp"), None),
        P(),
        P(("grp", "ep", "tp"), None),
        P(("grp", "ep", "tp"), None),
        P(("ep", "tp"), None, None),
        P(("ep", "tp"), None, None),
        P(("ep", "tp"), None, None),
        P(None, "tp"),
        P(None, "tp"),
        P("tp", None),
    )
    return jax.shard_map(
        local_of(mesh),
        mesh=mesh,
        in_specs=placed,
        out_specs=(P(("grp", "ep"), "tp", None), P(("grp", "ep", "tp"), None)),
        check_vma=False,
    )
```

```python
import functools
import jax
import jax.numpy as jnp
from jax import lax
from jax.experimental import pallas as pl
from jax.experimental.pallas import tpu as pltpu
from jax.sharding import PartitionSpec as P

MESH = pl.DeviceIdType.MESH
F32 = jnp.float32
BF16 = jnp.bfloat16
CAP = 2
GROUPS = 2
HALVES = 2
SENDS = 4
RETURNS = 4
SHARED = 4
AHEAD = 3

D = 4096
EXPERTS = 128
TOP_K = 2


def rms_rows(row_values, gain_vector):
    widened = row_values.astype(jnp.float32)
    inverse = lax.rsqrt(jnp.mean(widened * widened, axis=-1, keepdims=True) + 1e-06)
    return (widened * inverse * gain_vector).astype(jnp.bfloat16)


def attend(queries, key_vectors, values, forget_cum, query_gain, key_gain):
    query_norm = rms_rows(queries, query_gain)
    key_norm = rms_rows(key_vectors, key_gain)
    query_rows = query_norm.shape[0]
    head_count = query_norm.shape[1]
    head_size = query_norm.shape[2]
    first_query = lax.axis_index("ep") * query_rows
    query_positions = first_query + lax.iota(jnp.int32, query_rows)
    last_query = first_query + query_rows - 1
    query_cum = lax.dynamic_slice_in_dim(forget_cum, first_query, query_rows, 0).T
    scale_factor = head_size ** (-0.5)
    start_state = (
        jnp.full((head_count, query_rows), -1e30, jnp.float32),
        jnp.zeros((head_count, query_rows), jnp.float32),
        jnp.zeros((head_count, query_rows, head_size), jnp.float32),
    )
    key_part = lax.all_gather(key_norm, "ep", axis=0, tiled=True)
    value_part = lax.all_gather(values, "ep", axis=0, tiled=True)
    piece_rows = key_part.shape[0]

    def compute(inner_state):
        best_score, denominator, accumulated = inner_state
        cum_block = forget_cum.T
        scores = jnp.einsum(
            "qhd,khd->hqk", query_norm, key_part, preferred_element_type=jnp.float32
        )
        scores = scores * scale_factor + query_cum[:, :, None] - cum_block[:, None, :]
        key_positions = lax.iota(jnp.int32, piece_rows)
        allowed = (key_positions[None, :] <= query_positions[:, None])[None]
        scores = jnp.where(allowed, scores, -1e30)
        new_best = jnp.maximum(best_score, jnp.max(scores, axis=2))
        weights = jnp.where(allowed, jnp.exp(scores - new_best[:, :, None]), 0.0)
        denominator = jnp.sum(weights, axis=2)
        product = jnp.einsum(
            "hqk,khd->hqd",
            weights.astype(jnp.bfloat16),
            value_part,
            preferred_element_type=jnp.float32,
        )
        accumulated = product
        return (new_best, denominator, accumulated)

    best_score, denominator, accumulated = lax.cond(
        jnp.int32(0) <= last_query, compute, lambda inner_state: inner_state, start_state
    )
    return (accumulated / denominator[:, :, None]).transpose(1, 0, 2).astype(jnp.bfloat16)


def shared_expert(normed, shared_gate, shared_up, shared_down):
    row_count = normed.shape[0]
    whole_gate, whole_up, whole_down = (
        lax.all_gather(shared_gate, "tp", axis=1, tiled=True),
        lax.all_gather(shared_up, "tp", axis=1, tiled=True),
        lax.all_gather(shared_down, "tp", axis=0, tiled=True),
    )
    block_total = lax.axis_size("tp")
    gate_values = jnp.dot(normed, whole_gate, preferred_element_type=jnp.float32)
    upward = jnp.dot(normed, whole_up, preferred_element_type=jnp.float32)
    hidden_whole = (jax.nn.silu(gate_values) * upward).astype(jnp.bfloat16)
    part_width = whole_down.shape[0] // block_total
    hidden_blocks = hidden_whole.reshape(row_count, block_total, part_width)
    down_blocks = whole_down.reshape(block_total, part_width, whole_down.shape[1])
    partials = jnp.einsum(
        "rnp,npd->nrd", hidden_blocks, down_blocks, preferred_element_type=jnp.float32
    ).astype(jnp.bfloat16)
    return jnp.sum(partials.astype(jnp.float32), axis=0).astype(jnp.bfloat16)


def mixture(
    tokens,
    norm_gain,
    routes,
    route_weights,
    expert_gate,
    expert_up,
    expert_down,
    shared_gate,
    shared_up,
    shared_down,
):
    normed = rms_rows(tokens, norm_gain)
    row_count = tokens.shape[0]
    shared_out = shared_expert(normed, shared_gate, shared_up, shared_down)
    flat_routes = routes.reshape(-1)
    choice_count = flat_routes.shape[0]
    one_hot = (flat_routes[:, None] == lax.iota(jnp.int32, EXPERTS)[None, :]).astype(jnp.int32)
    slot_rank = jnp.sum((jnp.cumsum(one_hot, axis=0) - one_hot) * one_hot, axis=1)
    slot_index = slot_rank * EXPERTS + flat_routes
    slot_ids = lax.iota(jnp.int32, CAP * EXPERTS)
    matches = slot_index[None, :] == slot_ids[:, None]
    source_row = jnp.sum(
        jnp.where(matches, lax.iota(jnp.int32, choice_count)[None, :] // TOP_K, 0), axis=1
    )
    filled = jnp.any(matches, axis=1)
    outgoing = jnp.where(filled[:, None], normed[source_row], jnp.zeros((), jnp.bfloat16)).reshape(
        CAP, EXPERTS, D
    )
    arrived = lax.all_to_all(outgoing, ("ep", "tp"), split_axis=1, concat_axis=1, tiled=True)
    local_count = expert_gate.shape[0]
    grouped = arrived.reshape(CAP, -1, local_count, D)
    gate_values = jnp.einsum(
        "csed,edf->csef", grouped, expert_gate, preferred_element_type=jnp.float32
    )
    upward = jnp.einsum("csed,edf->csef", grouped, expert_up, preferred_element_type=jnp.float32)
    hidden = (jax.nn.silu(gate_values) * upward).astype(jnp.bfloat16)
    produced = (
        jnp.einsum("csef,efd->csed", hidden, expert_down, preferred_element_type=jnp.float32)
        .astype(jnp.bfloat16)
        .reshape(CAP, -1, D)
    )
    returned = lax.all_to_all(produced, ("ep", "tp"), split_axis=1, concat_axis=1, tiled=True)
    picked_rows = returned.reshape(CAP * EXPERTS, D)[slot_index].reshape(row_count, TOP_K, D)
    routed = jnp.sum(route_weights[:, :, None] * picked_rows.astype(jnp.float32), axis=1)
    return (shared_out.astype(jnp.float32) + routed).astype(jnp.bfloat16)


def local(
    queries,
    key_vectors,
    values,
    forget_cum,
    query_gain,
    key_gain,
    tokens,
    norm_gain,
    routes,
    route_weights,
    expert_gate,
    expert_up,
    expert_down,
    shared_gate,
    shared_up,
    shared_down,
):
    attended = attend(queries, key_vectors, values, forget_cum, query_gain, key_gain)
    routed_output = mixture(
        tokens,
        norm_gain,
        routes,
        route_weights,
        expert_gate,
        expert_up,
        expert_down,
        shared_gate,
        shared_up,
        shared_down,
    )
    return (attended, routed_output)


def rms_heads(wide, gain, heads):
    pieces = []
    for h in range(heads):
        part = wide[:, h, :]
        inverse = lax.rsqrt(jnp.mean(part * part, axis=-1, keepdims=True) + 1e-06)
        pieces.append((part * inverse * gain).astype(BF16))
    return jnp.concatenate(pieces, axis=1)


def iota(shape, axis):
    return lax.broadcasted_iota(jnp.int32, shape, axis)


def fused_kernel(
    n_ep,
    n_tp,
    heads,
    tokens_ref,
    gain_ref,
    routes_ref,
    weights_ref,
    q_ref,
    k_ref,
    v_ref,
    qg_ref,
    kg_ref,
    cum_ref,
    gate_ref,
    up_ref,
    down_ref,
    sg_ref,
    su_ref,
    sd_ref,
    att_ref,
    res_ref,
    tok,
    gain,
    routes,
    weights,
    q_in,
    k_in,
    v_in,
    q_gain,
    k_gain,
    cum,
    normed,
    pick,
    comb,
    gather,
    scatter,
    outgoing,
    x_buf,
    x_rows,
    wide_w,
    down_w,
    y_rows,
    y_buf,
    r_buf,
    sh_buf,
    total,
    qn,
    kv_buf,
    q_far,
    far_out,
    far_in,
    stat_out,
    stat_in,
    near_sum,
    in_sem,
    w_sem,
    x_send,
    x_recv,
    y_send,
    y_recv,
    sh_send,
    sh_recv,
    sh_own,
    sf_send,
    sf_recv,
    kv_send,
    kv_recv,
    q_send,
    q_recv,
    far_send,
    far_recv,
    credit,
):
    e_pos = lax.axis_index("ep")
    t_pos = lax.axis_index("tp")
    count = n_ep * n_tp
    me = e_pos * n_tp + t_pos
    local_count = gate_ref.shape[0]
    per = local_count // GROUPS
    hidden_width = gate_ref.shape[2]
    block = HALVES * per * CAP
    slots = count * block
    expert_rows = count * CAP
    group_rows = per * expert_rows
    rows, dim = tok.shape
    half = dim // HALVES
    x_wide = half // SENDS
    y_wide = half // RETURNS
    peer_rows = (count - 1) * block

    def device(i):
        return {"ep": i // n_tp, "tp": i % n_tp}

    barrier = pltpu.get_barrier_semaphore()

    def greet(i, carry):
        pl.semaphore_signal(
            barrier, inc=1, device_id=device((me + i) % count), device_id_type=MESH
        )
        return carry

    lax.fori_loop(1, count, greet, 0)
    inputs = [
        pltpu.make_async_copy(src, dst, in_sem.at[i])
        for i, (src, dst) in enumerate(
            (
                (routes_ref, routes),
                (tokens_ref, tok),
                (gain_ref, gain),
                (weights_ref, weights),
                (k_ref, k_in),
                (v_ref, v_in),
                (q_ref, q_in),
                (qg_ref, q_gain),
                (kg_ref, k_gain),
                (cum_ref, cum),
            )
        )
    ]
    for copy in inputs:
        copy.start()

    def weight_copies(g, e):
        n = g * per + e
        return (
            pltpu.make_async_copy(
                gate_ref.at[n], wide_w.at[e, :, pl.ds(0, hidden_width)], w_sem.at[e, 0]
            ),
            pltpu.make_async_copy(
                up_ref.at[n], wide_w.at[e, :, pl.ds(hidden_width, hidden_width)], w_sem.at[e, 1]
            ),
            pltpu.make_async_copy(down_ref.at[n], down_w.at[e], w_sem.at[e, 2]),
        )

    def first_weights(e, carry):
        for copy in weight_copies(0, e):
            copy.start()
        return carry

    shared_refs = (sg_ref, su_ref, sd_ref)
    part = sd_ref.shape[0]
    own_shared = [
        pltpu.make_async_copy(src, sh_buf.at[t_pos, pl.ds(j * part, part)], sh_own)
        for j, src in enumerate(shared_refs)
    ]

    inputs[0].wait()
    inputs[3].wait()
    lax.fori_loop(0, per, first_weights, 0)
    for copy in own_shared:
        copy.start()

    r = iota((slots, rows), 0)
    which_half = (r % block) // (per * CAP)
    before = jnp.where(iota((rows, rows), 0) < iota((rows, rows), 1), 1.0, 0.0).astype(BF16)

    def chosen(g):
        expert = (r // block) * local_count + g * per + (r % (per * CAP)) // CAP
        first = expert == routes[0:1, :]
        named = jnp.where(first | (expert == routes[1:2, :]), 1.0, 0.0)
        earlier = jnp.dot(named.astype(BF16), before, preferred_element_type=F32)
        return first, jnp.where(earlier == (r % CAP).astype(F32), named, 0.0)

    def fill_pick(g):
        _, hit = chosen(g)
        for h in range(HALVES):
            pick[g, :, h * rows : (h + 1) * rows] = jnp.where(which_half == h, hit, 0.0).astype(
                BF16
            )

    fill_pick(0)
    inputs[1].wait()
    inputs[2].wait()
    wide = tok[...].astype(F32)
    inverse = lax.rsqrt(jnp.mean(wide * wide, axis=-1, keepdims=True) + 1e-06)
    step = half // 4
    for h in range(HALVES):
        for c in range(4):
            cols = slice(h * half + c * step, h * half + (c + 1) * step)
            normed[h * rows : (h + 1) * rows, c * step : (c + 1) * step] = (
                tok[:, cols].astype(F32) * inverse * gain[:, cols]
            ).astype(BF16)
    pl.semaphore_wait(barrier, count - 1)

    def rows_of(i):
        return pl.ds(pl.multiple_of(i * block, block), block)

    beside = e_pos + 1 - 2 * (e_pos % 2)
    opposite = 1 - e_pos // 2
    inner = opposite + 1
    outer = opposite * (n_ep - 1)
    every = (inner, outer, beside, e_pos)

    def to_peers(src, dst, send_sem, recv_sem, planes):
        for e in planes:

            def send(j, carry):
                peer = e * n_tp + (t_pos + j) % n_tp
                pltpu.make_async_remote_copy(
                    src_ref=src.at[rows_of(peer)],
                    dst_ref=dst.at[rows_of(me)],
                    send_sem=send_sem,
                    recv_sem=recv_sem,
                    device_id=device(peer),
                    device_id_type=MESH,
                ).start()
                return carry

            lax.fori_loop(1 if e is e_pos else 0, n_tp, send, 0)

    def pick_rows(g, c):
        outgoing[g, c] = jnp.dot(
            pick[g], normed[:, c * x_wide : (c + 1) * x_wide], preferred_element_type=F32
        ).astype(BF16)
        x_buf[g, c, rows_of(me)] = outgoing[g, c, rows_of(me)]

    def dispatch(g, c):
        to_peers(outgoing.at[g, c], x_buf.at[g, c], x_send.at[g], x_recv.at[g, c], every)

    mate = t_pos + 1 - 2 * (t_pos % 2)
    across = (t_pos + 2) % n_tp
    sh_wide = dim // SHARED

    def shared_send(c):
        cols = pl.ds(c * sh_wide, sh_wide)
        for s, target in enumerate((mate, across)):
            for j, src in enumerate(shared_refs):
                pltpu.make_async_remote_copy(
                    src_ref=src.at[:, cols],
                    dst_ref=sh_buf.at[t_pos, pl.ds(j * part, part), cols],
                    send_sem=sh_send,
                    recv_sem=sh_recv.at[s],
                    device_id={"tp": target},
                    device_id_type=MESH,
                ).start()

    order = [(g, c) for g in range(GROUPS) for c in range(SENDS)]

    def arrived(n):
        g, c = order[n]
        away = x_buf.at[g, c, pl.ds(0, peer_rows)]
        pltpu.make_async_copy(away, away, x_recv.at[g, c]).wait()

    def exchange_credit():
        pl.semaphore_signal(
            credit,
            inc=1,
            device_id={"ep": n_ep - 1 - e_pos, "tp": t_pos},
            device_id_type=MESH,
        )
        pl.semaphore_wait(credit, 1)

    pick_rows(*order[0])
    for n in range(1, AHEAD):
        pick_rows(*order[n])
        dispatch(*order[n - 1])
    for n in range(AHEAD, SENDS):
        pick_rows(*order[n])
    dispatch(*order[AHEAD - 1])
    for g in range(1, GROUPS):
        fill_pick(g)
    shared_send(0)

    for copy in inputs[4:]:
        copy.wait()
    qn[...] = rms_heads(q_in[...].astype(F32), q_gain[...], heads)
    kv_buf[e_pos % 2, 0] = rms_heads(k_in[...].astype(F32), k_gain[...], heads)
    held = v_in[...].astype(F32)
    kv_buf[e_pos % 2, 1] = jnp.concatenate(
        [held[:, h, :].astype(BF16) for h in range(heads)], axis=1
    )

    @pl.when(e_pos % 2 == 0)
    def _():
        kv_buf[1] = jnp.zeros(kv_buf.shape[1:], BF16)

    for g in range(1, GROUPS):
        for c in range(SENDS):
            pick_rows(g, c)

    def kv_copy():
        return pltpu.make_async_remote_copy(
            src_ref=kv_buf.at[0],
            dst_ref=kv_buf.at[0],
            send_sem=kv_send,
            recv_sem=kv_recv,
            device_id={"ep": jnp.minimum(e_pos + 1, n_ep - 1)},
            device_id_type=MESH,
        )

    far_index = jnp.maximum(e_pos - 2, 0)

    def q_copy():
        return pltpu.make_async_remote_copy(
            src_ref=qn,
            dst_ref=q_far.at[far_index],
            send_sem=q_send,
            recv_sem=q_recv.at[far_index],
            device_id={"ep": 1},
            device_id_type=MESH,
        )

    big_row = iota((slots, HALVES * group_rows), 1)
    big_slot = iota((slots, HALVES * group_rows), 0)

    def slot_of(n):
        h = n // group_rows
        e = (n % group_rows) // expert_rows
        src = (n % expert_rows) // CAP
        return src * block + h * (per * CAP) + e * CAP + n % CAP

    scatter[...] = jnp.where(slot_of(big_row) == big_slot, 1.0, 0.0).astype(BF16)
    big_row = iota((HALVES * group_rows, slots), 0)
    big_slot = iota((HALVES * group_rows, slots), 1)
    gather[...] = jnp.where(slot_of(big_row) == big_slot, 1.0, 0.0).astype(BF16)

    for g in range(GROUPS):
        first, hit = chosen(g)
        weight = jnp.where(first, weights[0:1, :], weights[1:2, :]) * hit
        for h in range(HALVES):
            mine = jnp.where(which_half == h, weight, 0.0).T
            high = mine.astype(BF16)
            comb[g, h] = high
            comb[g, HALVES + h] = (mine - high.astype(F32)).astype(BF16)

    for n in range(SENDS):
        arrived(n)
        exchange_credit()
        if n + 1 < SENDS:
            dispatch(*order[n + AHEAD])
        else:
            for m in range(n + AHEAD, len(order)):
                dispatch(*order[m])
        if n == 0:

            @pl.when(e_pos % 2 == 0)
            def _():
                kv_copy().start()

            @pl.when(e_pos >= 2)
            def _():
                q_copy().start()

        if n == 2:
            shared_send(1)

    size = qn.shape[1] // heads
    contract = (((1,), (1,)), ((), ()))
    diagonal = iota((rows, rows), 0) == iota((rows, rows), 1)

    def column(row):
        return jnp.sum(jnp.where(diagonal, row, 0.0), axis=1, keepdims=True)

    def as_row(col):
        return jnp.sum(jnp.where(diagonal, col, 0.0), axis=0, keepdims=True)

    def span_of(h):
        return slice(h * size, (h + 1) * size)

    def attend_pair(h, q, query_start, key_start, allowed):
        query_span = pl.ds(pl.multiple_of(query_start, rows), rows)
        key_span = pl.ds(pl.multiple_of(key_start, 2 * rows), 2 * rows)
        scores = jnp.concatenate(
            [
                lax.dot_general(
                    q, kv_buf[b, 0, :, span_of(h)], contract, preferred_element_type=F32
                )
                for b in range(2)
            ],
            axis=1,
        )
        scores = (
            scores * (size**-0.5)
            + column(cum[h : h + 1, query_span])
            - cum[h : h + 1, key_span]
        )
        if allowed is not None:
            scores = jnp.where(allowed, scores, -1e30)
        top = jnp.max(scores, axis=1, keepdims=True)
        probs = jnp.exp(scores - top)
        if allowed is not None:
            probs = jnp.where(allowed, probs, 0.0)
        norm = jnp.sum(probs, axis=1, keepdims=True)
        probs = probs.astype(BF16)
        mixed = jnp.dot(
            probs[:, :rows], kv_buf[0, 1, :, span_of(h)], preferred_element_type=F32
        ) + jnp.dot(probs[:, rows:], kv_buf[1, 1, :, span_of(h)], preferred_element_type=F32)
        return top, norm, mixed

    def compute(g):
        for c in range(SENDS):
            ordered = jnp.dot(gather[...], x_buf[g, c], preferred_element_type=F32).astype(BF16)
            for h in range(HALVES):
                start = h * half + c * x_wide
                x_rows[:, start : start + x_wide] = ordered[
                    h * group_rows : (h + 1) * group_rows
                ]

        def one(e, carry):
            copies = weight_copies(g, e)
            span = pl.ds(pl.multiple_of(e * expert_rows, expert_rows), expert_rows)
            copies[0].wait()
            copies[1].wait()
            both = jnp.dot(x_rows[span], wide_w[e], preferred_element_type=F32)
            gate = both[:, :hidden_width]
            hidden = (gate / (1.0 + jnp.exp(-gate)) * both[:, hidden_width:]).astype(BF16)
            copies[2].wait()
            for h in range(HALVES):
                at = pl.ds(pl.multiple_of(h * group_rows + e * expert_rows, expert_rows), expert_rows)
                for c in range(2):
                    cols = slice(c * half // 2, (c + 1) * half // 2)
                    y_rows[at, cols] = jnp.dot(
                        hidden,
                        down_w[e, :, h * half + c * half // 2 : h * half + (c + 1) * half // 2],
                        preferred_element_type=F32,
                    ).astype(BF16)
            if g + 1 < GROUPS:
                for copy in weight_copies(g + 1, e):
                    copy.start()
            return carry

        lax.fori_loop(0, per, one, 0)

    def place(g, c):
        y_buf[g, c] = jnp.dot(
            scatter[...], y_rows[:, c * y_wide : (c + 1) * y_wide], preferred_element_type=F32
        ).astype(BF16)
        r_buf[g, c, rows_of(me)] = y_buf[g, c, rows_of(me)]

    def give(g, c, planes):
        arrival = c if g + 1 == GROUPS else RETURNS
        to_peers(y_buf.at[g, c], r_buf.at[g, c], y_send.at[g], y_recv.at[arrival], planes)

    compute(0)
    shared_send(2)
    for c in range(RETURNS):
        place(0, c)
    @pl.when(e_pos % 2 == 1)
    def _():
        kv_copy().wait_recv()

    at = (e_pos % 2) * rows + iota((rows, 2 * rows), 0)
    allowed = iota((rows, 2 * rows), 1) <= at
    near = [
        attend_pair(h, qn[:, span_of(h)], e_pos * rows, (e_pos // 2) * 2 * rows, allowed)
        for h in range(heads)
    ]
    for h in range(heads):
        near_sum[:, span_of(h)] = near[h][2]

    @pl.when(e_pos == 1)
    def _():
        for i in range(2):
            pltpu.make_async_copy(q_far.at[i], q_far.at[i], q_recv.at[i]).wait()
            for h in range(heads):
                top, norm, mixed = attend_pair(
                    h, q_far[i, :, span_of(h)], (2 + i) * rows, 0, None
                )
                far_out[i, :, span_of(h)] = mixed.astype(BF16)
                stat_out[i, h : h + 1] = as_row(top)
                stat_out[i, heads + h : heads + h + 1] = as_row(norm)

    def far_copies(i):
        return (
            pltpu.make_async_remote_copy(
                src_ref=far_out.at[i],
                dst_ref=far_in,
                send_sem=far_send.at[i, 0],
                recv_sem=far_recv.at[0],
                device_id={"ep": 2 + i},
                device_id_type=MESH,
            ),
            pltpu.make_async_remote_copy(
                src_ref=stat_out.at[i],
                dst_ref=stat_in,
                send_sem=far_send.at[i, 1],
                recv_sem=far_recv.at[1],
                device_id={"ep": 2 + i},
                device_id_type=MESH,
            ),
        )

    for n in range(SENDS, len(order)):
        arrived(n)
        if n == SENDS:

            @pl.when(e_pos == 1)
            def _():
                for i in range(2):
                    for copy in far_copies(i):
                        copy.start()

        if n + 2 == len(order):
            exchange_credit()
            give(0, 0, every)
    exchange_credit()
    for c in range(1, RETURNS):
        give(0, c, every)
    shared_send(3)
    compute(1)
    first_planes = (outer, beside, e_pos)
    place(1, 0)
    for c in range(1, RETURNS):
        place(1, c)
        give(1, c - 1, first_planes)

    @pl.when(e_pos < 2)
    def _():
        far_in[...] = jnp.zeros(far_in.shape, BF16)
        stat_in[0:heads] = jnp.full((heads, rows), -1e30, F32)
        stat_in[heads:] = jnp.zeros((stat_in.shape[0] - heads, rows), F32)

    give(1, RETURNS - 1, first_planes)
    for c in range(RETURNS):
        give(1, c, (inner,))

    def whole(i):
        return sh_buf.at[i]

    pltpu.make_async_copy(whole(across), whole(across), sh_recv.at[1]).wait()
    across_copy = pltpu.make_async_remote_copy(
        src_ref=whole(across),
        dst_ref=whole(across),
        send_sem=sf_send,
        recv_sem=sf_recv,
        device_id={"tp": mate},
        device_id_type=MESH,
    )
    across_copy.start()
    pltpu.make_async_copy(whole(t_pos), whole(t_pos), sh_own).wait()
    third = mate + 2 - 4 * (mate // 2)
    pltpu.make_async_copy(whole(mate), whole(mate), sh_recv.at[0]).wait()
    pltpu.make_async_copy(whole(third), whole(third), sf_recv).wait()
    hidden_parts = []
    for blk in range(n_tp):
        both = [
            sum(
                lax.dot_general(
                    normed[h * rows : (h + 1) * rows, :],
                    sh_buf[blk, j * part : (j + 1) * part, h * half : (h + 1) * half],
                    contract,
                    preferred_element_type=F32,
                )
                for h in range(HALVES)
            )
            for j in range(2)
        ]
        hidden_parts.append((both[0] / (1.0 + jnp.exp(-both[0])) * both[1]).astype(BF16))
    narrow = dim // 8
    for c in range(8):
        cols = slice(c * narrow, (c + 1) * narrow)
        summed = jnp.zeros((rows, narrow), F32)
        for blk in range(n_tp):
            piece = jnp.dot(
                hidden_parts[blk],
                sh_buf[blk, 2 * part : 3 * part, cols],
                preferred_element_type=F32,
            )
            summed += piece.astype(BF16).astype(F32)
        total[:, cols] = summed.astype(BF16).astype(F32)

    def returned(g, c):
        back = r_buf[g, c]
        for h in range(HALVES):
            cols = slice(h * half + c * y_wide, h * half + (c + 1) * y_wide)
            routed = jnp.dot(comb[g, h], back, preferred_element_type=F32) + jnp.dot(
                comb[g, HALVES + h], back, preferred_element_type=F32
            )
            if g + 1 < GROUPS:
                total[:, cols] += routed
            else:
                res_ref[:, cols] = (total[:, cols] + routed).astype(BF16)

    @pl.when(e_pos >= 2)
    def _():
        for copy in far_copies(0):
            copy.wait_recv()

    parts = []
    for h in range(heads):
        top, norm, _ = near[h]
        far_top = column(stat_in[h : h + 1])
        best = jnp.maximum(top, far_top)
        near_scale = jnp.exp(top - best)
        far_scale = jnp.exp(far_top - best)
        far_norm = column(stat_in[heads + h : heads + h + 1])
        mixed = near_sum[:, span_of(h)] * near_scale + far_in[:, span_of(h)].astype(F32) * far_scale
        parts.append(mixed / (norm * near_scale + far_norm * far_scale))
    att_ref[...] = jnp.stack(parts, axis=1).astype(BF16)

    away = r_buf.at[0, :, pl.ds(0, peer_rows)]
    pltpu.make_async_copy(away, away, y_recv.at[RETURNS]).wait()
    for c in range(RETURNS):
        returned(0, c)

    for c in range(RETURNS):
        away = r_buf.at[1, c, pl.ds(0, peer_rows)]
        pltpu.make_async_copy(away, away, y_recv.at[c]).wait()
        returned(1, c)

    for g in range(GROUPS):
        for buf, sem in ((x_buf, x_send), (y_buf, y_send)):
            away = buf.at[g, :, pl.ds(0, peer_rows)]
            pltpu.make_async_copy(away, away, sem.at[g]).wait()
    pair = sh_buf.at[pl.ds(0, 2)]
    pltpu.make_async_copy(pair, pair, sh_send).wait()
    across_copy.wait_send()

    @pl.when(e_pos % 2 == 0)
    def _():
        kv_copy().wait_send()

    @pl.when(e_pos >= 2)
    def _():
        q_copy().wait_send()

    @pl.when(e_pos == 1)
    def _():
        for i in range(2):
            for copy in far_copies(i):
                copy.wait_send()


def finish_kernel(att_ref, res_ref, att_out, res_out, sem):
    copies = [
        pltpu.make_async_copy(src, dst, sem.at[i])
        for i, (src, dst) in enumerate(((res_ref, res_out), (att_ref, att_out)))
    ]
    for copy in copies:
        copy.start()
    for copy in copies:
        copy.wait()


def fused_local(n_ep, n_tp, *args):
    (
        queries,
        key_vectors,
        values,
        forget_cum,
        query_gain,
        key_gain,
        tokens,
        norm_gain,
        routes,
        route_weights,
        expert_gate,
        expert_up,
        expert_down,
        shared_gate,
        shared_up,
        shared_down,
    ) = args
    rows, heads, size = queries.shape
    row_count, dim = tokens.shape
    local_count, _, hidden = expert_gate.shape
    count = n_ep * n_tp
    per = local_count // GROUPS
    slots = count * HALVES * per * CAP
    group_rows = count * per * CAP
    half = dim // HALVES
    part = shared_gate.shape[1]
    flat = heads * size
    hbm = pl.BlockSpec(memory_space=pltpu.HBM)
    sds = jax.ShapeDtypeStruct
    vmem = pltpu.VMEM
    dma = pltpu.SemaphoreType.DMA
    attended, routed = pl.pallas_call(
        functools.partial(fused_kernel, n_ep, n_tp, heads),
        out_shape=(vmem((rows, heads, size), BF16), vmem((row_count, dim), BF16)),
        in_specs=[hbm] * 16,
        out_specs=[pl.BlockSpec(memory_space=pltpu.VMEM)] * 2,
        scratch_shapes=[
            vmem((row_count, dim), BF16),
            vmem((1, dim), F32),
            vmem((TOP_K, row_count), jnp.int32),
            vmem((TOP_K, row_count), F32),
            vmem((rows, heads, size), BF16),
            vmem((rows, heads, size), BF16),
            vmem((rows, heads, size), BF16),
            vmem((1, size), F32),
            vmem((1, size), F32),
            vmem((heads, n_ep * rows), F32),
            vmem((HALVES * row_count, half), BF16),
            vmem((GROUPS, slots, HALVES * row_count), BF16),
            vmem((GROUPS, 2 * HALVES, row_count, slots), BF16),
            vmem((HALVES * group_rows, slots), BF16),
            vmem((slots, HALVES * group_rows), BF16),
            vmem((GROUPS, SENDS, slots, half // SENDS), BF16),
            vmem((GROUPS, SENDS, slots, half // SENDS), BF16),
            vmem((group_rows, dim), BF16),
            vmem((per, dim, 2 * hidden), BF16),
            vmem((per, hidden, dim), BF16),
            vmem((HALVES * group_rows, half), BF16),
            vmem((GROUPS, RETURNS, slots, half // RETURNS), BF16),
            vmem((GROUPS, RETURNS, slots, half // RETURNS), BF16),
            vmem((n_tp, 3 * part, dim), BF16),
            vmem((row_count, dim), F32),
            vmem((rows, flat), BF16),
            vmem((2, 2, rows, flat), BF16),
            vmem((2, rows, flat), BF16),
            vmem((2, rows, flat), BF16),
            vmem((rows, flat), BF16),
            vmem((2, 2 * heads, rows), F32),
            vmem((2 * heads, rows), F32),
            vmem((rows, flat), F32),
            dma((10,)),
            dma((per, 3)),
            dma((GROUPS,)),
            dma((GROUPS, SENDS)),
            dma((GROUPS,)),
            dma((RETURNS + 1,)),
            dma,
            dma((2,)),
            dma,
            dma,
            dma,
            dma,
            dma,
            dma,
            dma((2,)),
            dma((2, 2)),
            dma((2,)),
            pltpu.SemaphoreType.REGULAR,
        ],
        compiler_params=pltpu.CompilerParams(
            collective_id=0, has_side_effects=True, vmem_limit_bytes=60 * 1024 * 1024
        ),
        name="fused",
    )(
        tokens,
        norm_gain.reshape(1, dim),
        routes.T,
        route_weights.T,
        queries,
        key_vectors,
        values,
        query_gain.reshape(1, size),
        key_gain.reshape(1, size),
        forget_cum.T,
        expert_gate,
        expert_up,
        expert_down,
        shared_gate.T,
        shared_up.T,
        shared_down,
    )
    attended, routed = (
        pltpu.with_memory_space_constraint(a, pltpu.VMEM) for a in (attended, routed)
    )
    return pl.pallas_call(
        finish_kernel,
        out_shape=(sds((rows, heads, size), BF16), sds((row_count, dim), BF16)),
        in_specs=[pl.BlockSpec(memory_space=pltpu.VMEM)] * 2,
        out_specs=[hbm] * 2,
        scratch_shapes=[dma((2,))],
        name="finish",
    )(attended, routed)


def local_of(mesh):
    n_ep, n_tp = mesh.shape["ep"], mesh.shape["tp"]

    def run(*args):
        experts = args[10]
        block = CAP * experts.shape[0]
        if n_tp == 4 and n_ep == 4 and block % 16 == 0 and args[15].shape[0] % 16 == 0:
            return fused_local(n_ep, n_tp, *args)
        return local(*args)

    return run


def solution(mesh):
    placed = (
        P(("grp", "ep"), "tp", None),
        P(("grp", "ep"), "tp", None),
        P(("grp", "ep"), "tp", None),
        P("grp", "tp"),
        P(),
        P(),
        P(("grp", "ep", "tp"), None),
        P(),
        P(("grp", "ep", "tp"), None),
        P(("grp", "ep", "tp"), None),
        P(("ep", "tp"), None, None),
        P(("ep", "tp"), None, None),
        P(("ep", "tp"), None, None),
        P(None, "tp"),
        P(None, "tp"),
        P("tp", None),
    )
    return jax.shard_map(
        local_of(mesh),
        mesh=mesh,
        in_specs=placed,
        out_specs=(P(("grp", "ep"), "tp", None), P(("grp", "ep", "tp"), None)),
        check_vma=False,
    )
```

```python
import functools
import jax
import jax.numpy as jnp
from jax import lax
from jax.experimental import pallas as pl
from jax.experimental.pallas import tpu as pltpu
from jax.sharding import PartitionSpec as P

MESH = pl.DeviceIdType.MESH
F32 = jnp.float32
BF16 = jnp.bfloat16
CAP = 2
GROUPS = 2
HALVES = 2
SENDS = 4
RETURNS = 4
SHARED = 4
AHEAD = 3

D = 4096
EXPERTS = 128
TOP_K = 2


def rms_rows(row_values, gain_vector):
    widened = row_values.astype(jnp.float32)
    inverse = lax.rsqrt(jnp.mean(widened * widened, axis=-1, keepdims=True) + 1e-06)
    return (widened * inverse * gain_vector).astype(jnp.bfloat16)


def attend(queries, key_vectors, values, forget_cum, query_gain, key_gain):
    query_norm = rms_rows(queries, query_gain)
    key_norm = rms_rows(key_vectors, key_gain)
    query_rows = query_norm.shape[0]
    head_count = query_norm.shape[1]
    head_size = query_norm.shape[2]
    first_query = lax.axis_index("ep") * query_rows
    query_positions = first_query + lax.iota(jnp.int32, query_rows)
    last_query = first_query + query_rows - 1
    query_cum = lax.dynamic_slice_in_dim(forget_cum, first_query, query_rows, 0).T
    scale_factor = head_size ** (-0.5)
    start_state = (
        jnp.full((head_count, query_rows), -1e30, jnp.float32),
        jnp.zeros((head_count, query_rows), jnp.float32),
        jnp.zeros((head_count, query_rows, head_size), jnp.float32),
    )
    key_part = lax.all_gather(key_norm, "ep", axis=0, tiled=True)
    value_part = lax.all_gather(values, "ep", axis=0, tiled=True)
    piece_rows = key_part.shape[0]

    def compute(inner_state):
        best_score, denominator, accumulated = inner_state
        cum_block = forget_cum.T
        scores = jnp.einsum(
            "qhd,khd->hqk", query_norm, key_part, preferred_element_type=jnp.float32
        )
        scores = scores * scale_factor + query_cum[:, :, None] - cum_block[:, None, :]
        key_positions = lax.iota(jnp.int32, piece_rows)
        allowed = (key_positions[None, :] <= query_positions[:, None])[None]
        scores = jnp.where(allowed, scores, -1e30)
        new_best = jnp.maximum(best_score, jnp.max(scores, axis=2))
        weights = jnp.where(allowed, jnp.exp(scores - new_best[:, :, None]), 0.0)
        denominator = jnp.sum(weights, axis=2)
        product = jnp.einsum(
            "hqk,khd->hqd",
            weights.astype(jnp.bfloat16),
            value_part,
            preferred_element_type=jnp.float32,
        )
        accumulated = product
        return (new_best, denominator, accumulated)

    best_score, denominator, accumulated = lax.cond(
        jnp.int32(0) <= last_query, compute, lambda inner_state: inner_state, start_state
    )
    return (accumulated / denominator[:, :, None]).transpose(1, 0, 2).astype(jnp.bfloat16)


def shared_expert(normed, shared_gate, shared_up, shared_down):
    row_count = normed.shape[0]
    whole_gate, whole_up, whole_down = (
        lax.all_gather(shared_gate, "tp", axis=1, tiled=True),
        lax.all_gather(shared_up, "tp", axis=1, tiled=True),
        lax.all_gather(shared_down, "tp", axis=0, tiled=True),
    )
    block_total = lax.axis_size("tp")
    gate_values = jnp.dot(normed, whole_gate, preferred_element_type=jnp.float32)
    upward = jnp.dot(normed, whole_up, preferred_element_type=jnp.float32)
    hidden_whole = (jax.nn.silu(gate_values) * upward).astype(jnp.bfloat16)
    part_width = whole_down.shape[0] // block_total
    hidden_blocks = hidden_whole.reshape(row_count, block_total, part_width)
    down_blocks = whole_down.reshape(block_total, part_width, whole_down.shape[1])
    partials = jnp.einsum(
        "rnp,npd->nrd", hidden_blocks, down_blocks, preferred_element_type=jnp.float32
    ).astype(jnp.bfloat16)
    return jnp.sum(partials.astype(jnp.float32), axis=0).astype(jnp.bfloat16)


def mixture(
    tokens,
    norm_gain,
    routes,
    route_weights,
    expert_gate,
    expert_up,
    expert_down,
    shared_gate,
    shared_up,
    shared_down,
):
    normed = rms_rows(tokens, norm_gain)
    row_count = tokens.shape[0]
    shared_out = shared_expert(normed, shared_gate, shared_up, shared_down)
    flat_routes = routes.reshape(-1)
    choice_count = flat_routes.shape[0]
    one_hot = (flat_routes[:, None] == lax.iota(jnp.int32, EXPERTS)[None, :]).astype(jnp.int32)
    slot_rank = jnp.sum((jnp.cumsum(one_hot, axis=0) - one_hot) * one_hot, axis=1)
    slot_index = slot_rank * EXPERTS + flat_routes
    slot_ids = lax.iota(jnp.int32, CAP * EXPERTS)
    matches = slot_index[None, :] == slot_ids[:, None]
    source_row = jnp.sum(
        jnp.where(matches, lax.iota(jnp.int32, choice_count)[None, :] // TOP_K, 0), axis=1
    )
    filled = jnp.any(matches, axis=1)
    outgoing = jnp.where(filled[:, None], normed[source_row], jnp.zeros((), jnp.bfloat16)).reshape(
        CAP, EXPERTS, D
    )
    arrived = lax.all_to_all(outgoing, ("ep", "tp"), split_axis=1, concat_axis=1, tiled=True)
    local_count = expert_gate.shape[0]
    grouped = arrived.reshape(CAP, -1, local_count, D)
    gate_values = jnp.einsum(
        "csed,edf->csef", grouped, expert_gate, preferred_element_type=jnp.float32
    )
    upward = jnp.einsum("csed,edf->csef", grouped, expert_up, preferred_element_type=jnp.float32)
    hidden = (jax.nn.silu(gate_values) * upward).astype(jnp.bfloat16)
    produced = (
        jnp.einsum("csef,efd->csed", hidden, expert_down, preferred_element_type=jnp.float32)
        .astype(jnp.bfloat16)
        .reshape(CAP, -1, D)
    )
    returned = lax.all_to_all(produced, ("ep", "tp"), split_axis=1, concat_axis=1, tiled=True)
    picked_rows = returned.reshape(CAP * EXPERTS, D)[slot_index].reshape(row_count, TOP_K, D)
    routed = jnp.sum(route_weights[:, :, None] * picked_rows.astype(jnp.float32), axis=1)
    return (shared_out.astype(jnp.float32) + routed).astype(jnp.bfloat16)


def local(
    queries,
    key_vectors,
    values,
    forget_cum,
    query_gain,
    key_gain,
    tokens,
    norm_gain,
    routes,
    route_weights,
    expert_gate,
    expert_up,
    expert_down,
    shared_gate,
    shared_up,
    shared_down,
):
    attended = attend(queries, key_vectors, values, forget_cum, query_gain, key_gain)
    routed_output = mixture(
        tokens,
        norm_gain,
        routes,
        route_weights,
        expert_gate,
        expert_up,
        expert_down,
        shared_gate,
        shared_up,
        shared_down,
    )
    return (attended, routed_output)


def rms_heads(wide, gain, heads):
    pieces = []
    for h in range(heads):
        part = wide[:, h, :]
        inverse = lax.rsqrt(jnp.mean(part * part, axis=-1, keepdims=True) + 1e-06)
        pieces.append((part * inverse * gain).astype(BF16))
    return jnp.concatenate(pieces, axis=1)


def iota(shape, axis):
    return lax.broadcasted_iota(jnp.int32, shape, axis)


def fused_kernel(
    n_ep,
    n_tp,
    heads,
    tokens_ref,
    gain_ref,
    routes_ref,
    weights_ref,
    q_ref,
    k_ref,
    v_ref,
    qg_ref,
    kg_ref,
    cum_ref,
    gate_ref,
    up_ref,
    down_ref,
    sg_ref,
    su_ref,
    sd_ref,
    att_ref,
    res_ref,
    tok,
    gain,
    routes,
    weights,
    q_in,
    k_in,
    v_in,
    q_gain,
    k_gain,
    cum,
    normed,
    pick,
    comb,
    gather,
    scatter,
    outgoing,
    x_buf,
    x_rows,
    wide_w,
    down_w,
    y_rows,
    y_buf,
    r_buf,
    sh_buf,
    total,
    qn,
    kv_buf,
    q_far,
    far_out,
    far_in,
    stat_out,
    stat_in,
    near_sum,
    in_sem,
    w_sem,
    x_send,
    x_recv,
    y_send,
    y_recv,
    sh_send,
    sh_recv,
    sh_own,
    sf_send,
    sf_recv,
    kv_send,
    kv_recv,
    q_send,
    q_recv,
    far_send,
    far_recv,
    credit,
    ready,
    entered,
):
    e_pos = lax.axis_index("ep")
    t_pos = lax.axis_index("tp")
    count = n_ep * n_tp
    me = e_pos * n_tp + t_pos
    local_count = gate_ref.shape[0]
    per = local_count // GROUPS
    hidden_width = gate_ref.shape[2]
    block = HALVES * per * CAP
    slots = count * block
    expert_rows = count * CAP
    group_rows = per * expert_rows
    rows, dim = tok.shape
    half = dim // HALVES
    x_wide = half // SENDS
    y_wide = half // RETURNS
    peer_rows = (count - 1) * block

    def device(i):
        return {"ep": i // n_tp, "tp": i % n_tp}

    barrier = pltpu.get_barrier_semaphore()

    middle = (e_pos == 1) | (e_pos == 2)

    def greet_planes(semaphore, planes):
        for e in planes:

            def one(j, carry):
                pl.semaphore_signal(
                    semaphore,
                    inc=1,
                    device_id={"ep": e, "tp": (t_pos + j) % n_tp},
                    device_id_type=MESH,
                )
                return carry

            lax.fori_loop(1 if e is e_pos else 0, n_tp, one, 0)

    @pl.when(middle)
    def _():
        greet_planes(barrier, (n_ep - 1 - e_pos, e_pos))

    inputs = [
        pltpu.make_async_copy(src, dst, in_sem.at[i])
        for i, (src, dst) in enumerate(
            (
                (routes_ref, routes),
                (tokens_ref, tok),
                (gain_ref, gain),
                (weights_ref, weights),
                (k_ref, k_in),
                (v_ref, v_in),
                (q_ref, q_in),
                (qg_ref, q_gain),
                (kg_ref, k_gain),
                (cum_ref, cum),
            )
        )
    ]
    for copy in inputs:
        copy.start()

    def weight_copies(g, e):
        n = g * per + e
        return (
            pltpu.make_async_copy(
                gate_ref.at[n], wide_w.at[e, :, pl.ds(0, hidden_width)], w_sem.at[e, 0]
            ),
            pltpu.make_async_copy(
                up_ref.at[n], wide_w.at[e, :, pl.ds(hidden_width, hidden_width)], w_sem.at[e, 1]
            ),
            pltpu.make_async_copy(down_ref.at[n], down_w.at[e], w_sem.at[e, 2]),
        )

    def first_weights(e, carry):
        for copy in weight_copies(0, e):
            copy.start()
        return carry

    shared_refs = (sg_ref, su_ref, sd_ref)
    part = sd_ref.shape[0]
    own_shared = [
        pltpu.make_async_copy(src, sh_buf.at[t_pos, pl.ds(j * part, part)], sh_own)
        for j, src in enumerate(shared_refs)
    ]

    inputs[0].wait()
    inputs[3].wait()

    @pl.when(middle)
    def _():
        pl.semaphore_wait(barrier, 2 * n_tp - 1)
        greet_planes(barrier, (0, n_ep - 1))

    @pl.when(jnp.logical_not(middle))
    def _():
        pl.semaphore_wait(barrier, 2 * n_tp)
        greet_planes(ready, (1, 2))

    lax.fori_loop(0, per, first_weights, 0)
    for copy in own_shared:
        copy.start()

    r = iota((slots, rows), 0)
    which_half = (r % block) // (per * CAP)
    before = jnp.where(iota((rows, rows), 0) < iota((rows, rows), 1), 1.0, 0.0).astype(BF16)

    def chosen(g):
        expert = (r // block) * local_count + g * per + (r % (per * CAP)) // CAP
        first = expert == routes[0:1, :]
        named = jnp.where(first | (expert == routes[1:2, :]), 1.0, 0.0)
        earlier = jnp.dot(named.astype(BF16), before, preferred_element_type=F32)
        return first, jnp.where(earlier == (r % CAP).astype(F32), named, 0.0)

    def fill_pick(g):
        _, hit = chosen(g)
        for h in range(HALVES):
            pick[g, :, h * rows : (h + 1) * rows] = jnp.where(which_half == h, hit, 0.0).astype(
                BF16
            )

    fill_pick(0)
    inputs[1].wait()
    inputs[2].wait()
    wide = tok[...].astype(F32)
    inverse = lax.rsqrt(jnp.mean(wide * wide, axis=-1, keepdims=True) + 1e-06)
    step = half // 4
    for h in range(HALVES):
        for c in range(4):
            cols = slice(h * half + c * step, h * half + (c + 1) * step)
            normed[h * rows : (h + 1) * rows, c * step : (c + 1) * step] = (
                tok[:, cols].astype(F32) * inverse * gain[:, cols]
            ).astype(BF16)

    def rows_of(i):
        return pl.ds(pl.multiple_of(i * block, block), block)

    beside = e_pos + 1 - 2 * (e_pos % 2)
    opposite = 1 - e_pos // 2
    inner = opposite + 1
    outer = opposite * (n_ep - 1)
    every = (inner, outer, beside, e_pos)

    def to_peers(src, dst, send_sem, recv_sem, planes):
        for e in planes:

            def send(j, carry):
                peer = e * n_tp + (t_pos + j) % n_tp
                pltpu.make_async_remote_copy(
                    src_ref=src.at[rows_of(peer)],
                    dst_ref=dst.at[rows_of(me)],
                    send_sem=send_sem,
                    recv_sem=recv_sem,
                    device_id=device(peer),
                    device_id_type=MESH,
                ).start()
                return carry

            lax.fori_loop(1 if e is e_pos else 0, n_tp, send, 0)

    def pick_rows(g, c):
        outgoing[g, c] = jnp.dot(
            pick[g], normed[:, c * x_wide : (c + 1) * x_wide], preferred_element_type=F32
        ).astype(BF16)
        x_buf[g, c, rows_of(me)] = outgoing[g, c, rows_of(me)]

    def dispatch(g, c, planes=every):
        to_peers(outgoing.at[g, c], x_buf.at[g, c], x_send.at[g], x_recv.at[g, c], planes)

    mate = t_pos + 1 - 2 * (t_pos % 2)
    across = (t_pos + 2) % n_tp
    sh_wide = dim // SHARED

    def shared_send(c):
        cols = pl.ds(c * sh_wide, sh_wide)
        for s, target in enumerate((mate, across)):
            for j, src in enumerate(shared_refs):
                pltpu.make_async_remote_copy(
                    src_ref=src.at[:, cols],
                    dst_ref=sh_buf.at[t_pos, pl.ds(j * part, part), cols],
                    send_sem=sh_send,
                    recv_sem=sh_recv.at[s],
                    device_id={"tp": target},
                    device_id_type=MESH,
                ).start()

    order = [(g, c) for g in range(GROUPS) for c in range(SENDS)]

    def arrived(n):
        g, c = order[n]
        away = x_buf.at[g, c, pl.ds(0, peer_rows)]
        pltpu.make_async_copy(away, away, x_recv.at[g, c]).wait()

    def exchange_credit():
        pl.semaphore_signal(
            credit,
            inc=1,
            device_id={"ep": n_ep - 1 - e_pos, "tp": t_pos},
            device_id_type=MESH,
        )
        pl.semaphore_wait(credit, 1)

    pick_rows(*order[0])
    for n in range(1, SENDS):
        pick_rows(*order[n])
        if n <= AHEAD:

            @pl.when(middle)
            def _():
                dispatch(*order[n - 1], (inner, e_pos))

    @pl.when(middle)
    def _():
        pl.semaphore_wait(ready, 2 * n_tp)
        pl.semaphore_signal(
            entered, inc=1, device_id={"ep": beside, "tp": t_pos}, device_id_type=MESH
        )
        for n in range(AHEAD):
            dispatch(*order[n], (outer, beside))

    @pl.when(jnp.logical_not(middle))
    def _():
        for n in range(AHEAD):
            dispatch(*order[n], (inner, beside))
        pl.semaphore_wait(entered, 1)
        for n in range(AHEAD):
            dispatch(*order[n], (outer, e_pos))

    for g in range(1, GROUPS):
        fill_pick(g)
    shared_send(0)

    for copy in inputs[4:]:
        copy.wait()
    qn[...] = rms_heads(q_in[...].astype(F32), q_gain[...], heads)
    kv_buf[e_pos % 2, 0] = rms_heads(k_in[...].astype(F32), k_gain[...], heads)
    held = v_in[...].astype(F32)
    kv_buf[e_pos % 2, 1] = jnp.concatenate(
        [held[:, h, :].astype(BF16) for h in range(heads)], axis=1
    )

    @pl.when(e_pos % 2 == 0)
    def _():
        kv_buf[1] = jnp.zeros(kv_buf.shape[1:], BF16)

    for g in range(1, GROUPS):
        for c in range(SENDS):
            pick_rows(g, c)

    def kv_copy():
        return pltpu.make_async_remote_copy(
            src_ref=kv_buf.at[0],
            dst_ref=kv_buf.at[0],
            send_sem=kv_send,
            recv_sem=kv_recv,
            device_id={"ep": jnp.minimum(e_pos + 1, n_ep - 1)},
            device_id_type=MESH,
        )

    far_index = jnp.maximum(e_pos - 2, 0)

    def q_copy():
        return pltpu.make_async_remote_copy(
            src_ref=qn,
            dst_ref=q_far.at[far_index],
            send_sem=q_send,
            recv_sem=q_recv.at[far_index],
            device_id={"ep": 1},
            device_id_type=MESH,
        )

    big_row = iota((slots, HALVES * group_rows), 1)
    big_slot = iota((slots, HALVES * group_rows), 0)

    def slot_of(n):
        h = n // group_rows
        e = (n % group_rows) // expert_rows
        src = (n % expert_rows) // CAP
        return src * block + h * (per * CAP) + e * CAP + n % CAP

    scatter[...] = jnp.where(slot_of(big_row) == big_slot, 1.0, 0.0).astype(BF16)
    big_row = iota((HALVES * group_rows, slots), 0)
    big_slot = iota((HALVES * group_rows, slots), 1)
    gather[...] = jnp.where(slot_of(big_row) == big_slot, 1.0, 0.0).astype(BF16)

    for g in range(GROUPS):
        first, hit = chosen(g)
        weight = jnp.where(first, weights[0:1, :], weights[1:2, :]) * hit
        for h in range(HALVES):
            mine = jnp.where(which_half == h, weight, 0.0).T
            high = mine.astype(BF16)
            comb[g, h] = high
            comb[g, HALVES + h] = (mine - high.astype(F32)).astype(BF16)

    for n in range(SENDS):
        arrived(n)
        exchange_credit()
        if n + 1 < SENDS:
            dispatch(*order[n + AHEAD])
        else:
            for m in range(n + AHEAD, len(order)):
                dispatch(*order[m])
        if n == 0:

            @pl.when(e_pos % 2 == 0)
            def _():
                kv_copy().start()

            @pl.when(e_pos >= 2)
            def _():
                q_copy().start()

        if n == 2:
            shared_send(1)

    size = qn.shape[1] // heads
    contract = (((1,), (1,)), ((), ()))
    diagonal = iota((rows, rows), 0) == iota((rows, rows), 1)

    def column(row):
        return jnp.sum(jnp.where(diagonal, row, 0.0), axis=1, keepdims=True)

    def as_row(col):
        return jnp.sum(jnp.where(diagonal, col, 0.0), axis=0, keepdims=True)

    def span_of(h):
        return slice(h * size, (h + 1) * size)

    def attend_pair(h, q, query_start, key_start, allowed):
        query_span = pl.ds(pl.multiple_of(query_start, rows), rows)
        key_span = pl.ds(pl.multiple_of(key_start, 2 * rows), 2 * rows)
        scores = jnp.concatenate(
            [
                lax.dot_general(
                    q, kv_buf[b, 0, :, span_of(h)], contract, preferred_element_type=F32
                )
                for b in range(2)
            ],
            axis=1,
        )
        scores = (
            scores * (size**-0.5)
            + column(cum[h : h + 1, query_span])
            - cum[h : h + 1, key_span]
        )
        if allowed is not None:
            scores = jnp.where(allowed, scores, -1e30)
        top = jnp.max(scores, axis=1, keepdims=True)
        probs = jnp.exp(scores - top)
        if allowed is not None:
            probs = jnp.where(allowed, probs, 0.0)
        norm = jnp.sum(probs, axis=1, keepdims=True)
        probs = probs.astype(BF16)
        mixed = jnp.dot(
            probs[:, :rows], kv_buf[0, 1, :, span_of(h)], preferred_element_type=F32
        ) + jnp.dot(probs[:, rows:], kv_buf[1, 1, :, span_of(h)], preferred_element_type=F32)
        return top, norm, mixed

    def compute(g):
        for c in range(SENDS):
            ordered = jnp.dot(gather[...], x_buf[g, c], preferred_element_type=F32).astype(BF16)
            for h in range(HALVES):
                start = h * half + c * x_wide
                x_rows[:, start : start + x_wide] = ordered[
                    h * group_rows : (h + 1) * group_rows
                ]

        def one(e, carry):
            copies = weight_copies(g, e)
            span = pl.ds(pl.multiple_of(e * expert_rows, expert_rows), expert_rows)
            copies[0].wait()
            copies[1].wait()
            both = jnp.dot(x_rows[span], wide_w[e], preferred_element_type=F32)
            gate = both[:, :hidden_width]
            hidden = (gate / (1.0 + jnp.exp(-gate)) * both[:, hidden_width:]).astype(BF16)
            copies[2].wait()
            for h in range(HALVES):
                at = pl.ds(pl.multiple_of(h * group_rows + e * expert_rows, expert_rows), expert_rows)
                for c in range(2):
                    cols = slice(c * half // 2, (c + 1) * half // 2)
                    y_rows[at, cols] = jnp.dot(
                        hidden,
                        down_w[e, :, h * half + c * half // 2 : h * half + (c + 1) * half // 2],
                        preferred_element_type=F32,
                    ).astype(BF16)
            if g + 1 < GROUPS:
                for copy in weight_copies(g + 1, e):
                    copy.start()
            return carry

        lax.fori_loop(0, per, one, 0)

    def place(g, c):
        y_buf[g, c] = jnp.dot(
            scatter[...], y_rows[:, c * y_wide : (c + 1) * y_wide], preferred_element_type=F32
        ).astype(BF16)
        r_buf[g, c, rows_of(me)] = y_buf[g, c, rows_of(me)]

    def give(g, c, planes):
        arrival = c if g + 1 == GROUPS else RETURNS
        to_peers(y_buf.at[g, c], r_buf.at[g, c], y_send.at[g], y_recv.at[arrival], planes)

    compute(0)
    shared_send(2)
    for c in range(RETURNS):
        place(0, c)
    @pl.when(e_pos % 2 == 1)
    def _():
        kv_copy().wait_recv()

    at = (e_pos % 2) * rows + iota((rows, 2 * rows), 0)
    allowed = iota((rows, 2 * rows), 1) <= at
    near = [
        attend_pair(h, qn[:, span_of(h)], e_pos * rows, (e_pos // 2) * 2 * rows, allowed)
        for h in range(heads)
    ]
    for h in range(heads):
        near_sum[:, span_of(h)] = near[h][2]

    @pl.when(e_pos == 1)
    def _():
        for i in range(2):
            pltpu.make_async_copy(q_far.at[i], q_far.at[i], q_recv.at[i]).wait()
            for h in range(heads):
                top, norm, mixed = attend_pair(
                    h, q_far[i, :, span_of(h)], (2 + i) * rows, 0, None
                )
                far_out[i, :, span_of(h)] = mixed.astype(BF16)
                stat_out[i, h : h + 1] = as_row(top)
                stat_out[i, heads + h : heads + h + 1] = as_row(norm)

    def far_copies(i):
        return (
            pltpu.make_async_remote_copy(
                src_ref=far_out.at[i],
                dst_ref=far_in,
                send_sem=far_send.at[i, 0],
                recv_sem=far_recv.at[0],
                device_id={"ep": 2 + i},
                device_id_type=MESH,
            ),
            pltpu.make_async_remote_copy(
                src_ref=stat_out.at[i],
                dst_ref=stat_in,
                send_sem=far_send.at[i, 1],
                recv_sem=far_recv.at[1],
                device_id={"ep": 2 + i},
                device_id_type=MESH,
            ),
        )

    for n in range(SENDS, len(order)):
        arrived(n)
        if n == SENDS:

            @pl.when(e_pos == 1)
            def _():
                for i in range(2):
                    for copy in far_copies(i):
                        copy.start()

        if n + 2 == len(order):
            exchange_credit()
            give(0, 0, every)
    exchange_credit()
    for c in range(1, RETURNS):
        give(0, c, every)
    shared_send(3)
    compute(1)
    first_planes = (outer, beside, e_pos)
    place(1, 0)
    for c in range(1, RETURNS):
        place(1, c)
        give(1, c - 1, first_planes)

    @pl.when(e_pos < 2)
    def _():
        far_in[...] = jnp.zeros(far_in.shape, BF16)
        stat_in[0:heads] = jnp.full((heads, rows), -1e30, F32)
        stat_in[heads:] = jnp.zeros((stat_in.shape[0] - heads, rows), F32)

    give(1, RETURNS - 1, first_planes)
    for c in range(RETURNS):
        give(1, c, (inner,))

    def whole(i):
        return sh_buf.at[i]

    pltpu.make_async_copy(whole(across), whole(across), sh_recv.at[1]).wait()
    across_copy = pltpu.make_async_remote_copy(
        src_ref=whole(across),
        dst_ref=whole(across),
        send_sem=sf_send,
        recv_sem=sf_recv,
        device_id={"tp": mate},
        device_id_type=MESH,
    )
    across_copy.start()
    pltpu.make_async_copy(whole(t_pos), whole(t_pos), sh_own).wait()
    third = mate + 2 - 4 * (mate // 2)
    pltpu.make_async_copy(whole(mate), whole(mate), sh_recv.at[0]).wait()
    pltpu.make_async_copy(whole(third), whole(third), sf_recv).wait()
    hidden_parts = []
    for blk in range(n_tp):
        both = [
            sum(
                lax.dot_general(
                    normed[h * rows : (h + 1) * rows, :],
                    sh_buf[blk, j * part : (j + 1) * part, h * half : (h + 1) * half],
                    contract,
                    preferred_element_type=F32,
                )
                for h in range(HALVES)
            )
            for j in range(2)
        ]
        hidden_parts.append((both[0] / (1.0 + jnp.exp(-both[0])) * both[1]).astype(BF16))
    narrow = dim // 8
    for c in range(8):
        cols = slice(c * narrow, (c + 1) * narrow)
        summed = jnp.zeros((rows, narrow), F32)
        for blk in range(n_tp):
            piece = jnp.dot(
                hidden_parts[blk],
                sh_buf[blk, 2 * part : 3 * part, cols],
                preferred_element_type=F32,
            )
            summed += piece.astype(BF16).astype(F32)
        total[:, cols] = summed.astype(BF16).astype(F32)

    def returned(g, c):
        back = r_buf[g, c]
        for h in range(HALVES):
            cols = slice(h * half + c * y_wide, h * half + (c + 1) * y_wide)
            routed = jnp.dot(comb[g, h], back, preferred_element_type=F32) + jnp.dot(
                comb[g, HALVES + h], back, preferred_element_type=F32
            )
            if g + 1 < GROUPS:
                total[:, cols] += routed
            else:
                res_ref[:, cols] = (total[:, cols] + routed).astype(BF16)

    @pl.when(e_pos >= 2)
    def _():
        for copy in far_copies(0):
            copy.wait_recv()

    parts = []
    for h in range(heads):
        top, norm, _ = near[h]
        far_top = column(stat_in[h : h + 1])
        best = jnp.maximum(top, far_top)
        near_scale = jnp.exp(top - best)
        far_scale = jnp.exp(far_top - best)
        far_norm = column(stat_in[heads + h : heads + h + 1])
        mixed = near_sum[:, span_of(h)] * near_scale + far_in[:, span_of(h)].astype(F32) * far_scale
        parts.append(mixed / (norm * near_scale + far_norm * far_scale))
    att_ref[...] = jnp.stack(parts, axis=1).astype(BF16)

    away = r_buf.at[0, :, pl.ds(0, peer_rows)]
    pltpu.make_async_copy(away, away, y_recv.at[RETURNS]).wait()
    for c in range(RETURNS):
        returned(0, c)

    for c in range(RETURNS):
        away = r_buf.at[1, c, pl.ds(0, peer_rows)]
        pltpu.make_async_copy(away, away, y_recv.at[c]).wait()
        returned(1, c)

    for g in range(GROUPS):
        for buf, sem in ((x_buf, x_send), (y_buf, y_send)):
            away = buf.at[g, :, pl.ds(0, peer_rows)]
            pltpu.make_async_copy(away, away, sem.at[g]).wait()
    pair = sh_buf.at[pl.ds(0, 2)]
    pltpu.make_async_copy(pair, pair, sh_send).wait()
    across_copy.wait_send()

    @pl.when(e_pos % 2 == 0)
    def _():
        kv_copy().wait_send()

    @pl.when(e_pos >= 2)
    def _():
        q_copy().wait_send()

    @pl.when(e_pos == 1)
    def _():
        for i in range(2):
            for copy in far_copies(i):
                copy.wait_send()


def finish_kernel(att_ref, res_ref, att_out, res_out, sem):
    copies = [
        pltpu.make_async_copy(src, dst, sem.at[i])
        for i, (src, dst) in enumerate(((res_ref, res_out), (att_ref, att_out)))
    ]
    for copy in copies:
        copy.start()
    for copy in copies:
        copy.wait()


def fused_local(n_ep, n_tp, *args):
    (
        queries,
        key_vectors,
        values,
        forget_cum,
        query_gain,
        key_gain,
        tokens,
        norm_gain,
        routes,
        route_weights,
        expert_gate,
        expert_up,
        expert_down,
        shared_gate,
        shared_up,
        shared_down,
    ) = args
    rows, heads, size = queries.shape
    row_count, dim = tokens.shape
    local_count, _, hidden = expert_gate.shape
    count = n_ep * n_tp
    per = local_count // GROUPS
    slots = count * HALVES * per * CAP
    group_rows = count * per * CAP
    half = dim // HALVES
    part = shared_gate.shape[1]
    flat = heads * size
    hbm = pl.BlockSpec(memory_space=pltpu.HBM)
    sds = jax.ShapeDtypeStruct
    vmem = pltpu.VMEM
    dma = pltpu.SemaphoreType.DMA
    attended, routed = pl.pallas_call(
        functools.partial(fused_kernel, n_ep, n_tp, heads),
        out_shape=(vmem((rows, heads, size), BF16), vmem((row_count, dim), BF16)),
        in_specs=[hbm] * 16,
        out_specs=[pl.BlockSpec(memory_space=pltpu.VMEM)] * 2,
        scratch_shapes=[
            vmem((row_count, dim), BF16),
            vmem((1, dim), F32),
            vmem((TOP_K, row_count), jnp.int32),
            vmem((TOP_K, row_count), F32),
            vmem((rows, heads, size), BF16),
            vmem((rows, heads, size), BF16),
            vmem((rows, heads, size), BF16),
            vmem((1, size), F32),
            vmem((1, size), F32),
            vmem((heads, n_ep * rows), F32),
            vmem((HALVES * row_count, half), BF16),
            vmem((GROUPS, slots, HALVES * row_count), BF16),
            vmem((GROUPS, 2 * HALVES, row_count, slots), BF16),
            vmem((HALVES * group_rows, slots), BF16),
            vmem((slots, HALVES * group_rows), BF16),
            vmem((GROUPS, SENDS, slots, half // SENDS), BF16),
            vmem((GROUPS, SENDS, slots, half // SENDS), BF16),
            vmem((group_rows, dim), BF16),
            vmem((per, dim, 2 * hidden), BF16),
            vmem((per, hidden, dim), BF16),
            vmem((HALVES * group_rows, half), BF16),
            vmem((GROUPS, RETURNS, slots, half // RETURNS), BF16),
            vmem((GROUPS, RETURNS, slots, half // RETURNS), BF16),
            vmem((n_tp, 3 * part, dim), BF16),
            vmem((row_count, dim), F32),
            vmem((rows, flat), BF16),
            vmem((2, 2, rows, flat), BF16),
            vmem((2, rows, flat), BF16),
            vmem((2, rows, flat), BF16),
            vmem((rows, flat), BF16),
            vmem((2, 2 * heads, rows), F32),
            vmem((2 * heads, rows), F32),
            vmem((rows, flat), F32),
            dma((10,)),
            dma((per, 3)),
            dma((GROUPS,)),
            dma((GROUPS, SENDS)),
            dma((GROUPS,)),
            dma((RETURNS + 1,)),
            dma,
            dma((2,)),
            dma,
            dma,
            dma,
            dma,
            dma,
            dma,
            dma((2,)),
            dma((2, 2)),
            dma((2,)),
            pltpu.SemaphoreType.REGULAR,
            pltpu.SemaphoreType.REGULAR,
            pltpu.SemaphoreType.REGULAR,
        ],
        compiler_params=pltpu.CompilerParams(
            collective_id=0, has_side_effects=True, vmem_limit_bytes=60 * 1024 * 1024
        ),
        name="fused",
    )(
        tokens,
        norm_gain.reshape(1, dim),
        routes.T,
        route_weights.T,
        queries,
        key_vectors,
        values,
        query_gain.reshape(1, size),
        key_gain.reshape(1, size),
        forget_cum.T,
        expert_gate,
        expert_up,
        expert_down,
        shared_gate.T,
        shared_up.T,
        shared_down,
    )
    attended, routed = (
        pltpu.with_memory_space_constraint(a, pltpu.VMEM) for a in (attended, routed)
    )
    return pl.pallas_call(
        finish_kernel,
        out_shape=(sds((rows, heads, size), BF16), sds((row_count, dim), BF16)),
        in_specs=[pl.BlockSpec(memory_space=pltpu.VMEM)] * 2,
        out_specs=[hbm] * 2,
        scratch_shapes=[dma((2,))],
        name="finish",
    )(attended, routed)


def local_of(mesh):
    n_ep, n_tp = mesh.shape["ep"], mesh.shape["tp"]

    def run(*args):
        experts = args[10]
        block = CAP * experts.shape[0]
        if n_tp == 4 and n_ep == 4 and block % 16 == 0 and args[15].shape[0] % 16 == 0:
            return fused_local(n_ep, n_tp, *args)
        return local(*args)

    return run


def solution(mesh):
    placed = (
        P(("grp", "ep"), "tp", None),
        P(("grp", "ep"), "tp", None),
        P(("grp", "ep"), "tp", None),
        P("grp", "tp"),
        P(),
        P(),
        P(("grp", "ep", "tp"), None),
        P(),
        P(("grp", "ep", "tp"), None),
        P(("grp", "ep", "tp"), None),
        P(("ep", "tp"), None, None),
        P(("ep", "tp"), None, None),
        P(("ep", "tp"), None, None),
        P(None, "tp"),
        P(None, "tp"),
        P("tp", None),
    )
    return jax.shard_map(
        local_of(mesh),
        mesh=mesh,
        in_specs=placed,
        out_specs=(P(("grp", "ep"), "tp", None), P(("grp", "ep", "tp"), None)),
        check_vma=False,
    )
```
